32 devices in a mesh: fs: 8 (over z, y), tp: 4 (over x, core).
Axes of the slice: x: 2, y: 2, z: 4, core: 2. Of those that a mesh axis runs over, the one named last changes fastest.
Arguments:
- tokens: bfloat16 [8192, 2048], P('fs'), may hold values from -6 to 6
- norm_gain: float32 [2048], P('fs'), may hold values from 0.1 to 1.9
- gate_train: float32 [8, 2048, 768], P(None, 'fs', 'tp'), may hold values from -0.125 to 0.125
- up_train: float32 [8, 2048, 768], P(None, 'fs', 'tp'), may hold values from -0.125 to 0.125
- down_train: float32 [8, 768, 2048], P(None, 'fs', 'tp'), may hold values from -0.21875 to 0.21875
- expert_ids: int32 [8192, 2], P('fs'), may hold values from 0 to 7, all different within a row; in each aligned block of 1024 rows (0 to 1023, 1024 to 2047, ...) at most 512 rows name the same one
- route_weights: float32 [8192, 2], P('fs'), may hold values from 0.1 to 1
Outputs:
- gate_serve: bfloat16 [8, 2048, 768], P('fs', None, 'tp')
- up_serve: bfloat16 [8, 2048, 768], P('fs', None, 'tp')
- down_serve: bfloat16 [8, 768, 2048], P('fs', 'tp')
- mixed: bfloat16 [8192, 2048], P('fs', 'tp')
The draws below stay inside these ranges and needn't reach their ends.
Inputs may be any that keep to these rules, and one draw needn't show every extreme that they name: `expert_ids`: each row names 2 different experts. Within each aligned block of 1024 rows no expert is named more than 512 times, and in every block some expert is named exactly 512 times; every expert is named somewhere.
All inputs are finite; a program needn't handle non-finite values.
Results may differ from the reference program's by a relative error of at most 0.011.
Values may be sent and summed in bfloat16 or wider, within the bound.
A program may use at most 128 MiB of HBM per device.

```python
import math
import jax
import jax.numpy as jnp
import numpy as np
from jax import lax

D = 2048
FF = 768
TOP = 2
TOK_DEV = 1024
EXPERTS = 8
CAP = 512
TOKENS = 8192
N_FS = 8
N_TP = 4


def shard_levels(key, shape, shards, least, top_value):
    loudness = 1.0
    for axis_at, parts in shards:
        draws = jax.random.uniform(jax.random.fold_in(jax.random.fold_in(key, 6), axis_at), (parts,), jnp.float32, least / len(shards), top_value / len(shards))
        loudness = loudness * jnp.repeat(jnp.exp(draws), shape[axis_at] // parts).reshape((-1,) + (1,) * (len(shape) - 1 - axis_at))
    return loudness


def shared_out(own_key, own, number, rows, number_of, top, limit, lean):
    ranking = jax.random.permutation(own_key, number_of)
    heavy_load, ordinary = portions_of(number_of, rows * top, limit, lean, True), portions_of(number_of, rows * top, limit, lean, False)
    places = jnp.arange(number_of)

    def named(sizes, offset_by):
        used = int((sizes > 0).sum())
        fixed = max(1, used // 4)
        moved = fixed + (places - fixed + offset_by * (used - fixed)) % max(1, number_of - fixed)
        return jnp.zeros((number_of,), jnp.int32).at[ranking[jnp.where(places < fixed, places, moved)]].set(jnp.asarray(sizes, jnp.int32))

    sizes = jnp.where(number % 4 == 0, named(heavy_load, number // 4), named(ordinary, number - number // 4 - 1))
    mixed = jax.random.permutation(jax.random.fold_in(own, 3), number_of)
    source_of, sink = mixed[0:number_of // 2 * 2:2], mixed[1:number_of // 2 * 2:2]
    slack = jnp.minimum(sizes[source_of] - 1, limit - sizes[sink]) // 2
    slack = jnp.where((source_of == ranking[0]) | (sink == ranking[0]) | (sizes[sink] == 0), 0, jnp.maximum(slack, 0))
    moved = jax.random.randint(jax.random.fold_in(own, 4), (number_of // 2,), 0, 1 << 20) % (slack + 1)
    sizes = sizes.at[source_of].add(-moved).at[sink].add(moved)
    items = jnp.searchsorted(jnp.cumsum(sizes), jnp.arange(rows * top), side="right").astype(jnp.int32)
    table = items.reshape(top, rows).T
    table = table[jax.random.permutation(jax.random.fold_in(own, 1), rows)]
    offset_by = jax.random.randint(jax.random.fold_in(own, 2), (rows, 1), 0, top)
    return jnp.take_along_axis(table, (jnp.arange(top)[None, :] + offset_by) % top, axis=1)


def portions_of(number_of, total, limit, slope, full):
    portions = [(1 << 20) // math.isqrt(standing ** slope) + 1 for standing in range(1, number_of + 1)]
    largest = limit if full else min(limit, max(-(-total // number_of), total * portions[0] // sum(portions)))
    least = 1 if total - largest >= number_of - 1 else 0
    counts, rest = [largest] + [least] * (number_of - 1), total - largest - least * (number_of - 1)
    while rest > 0:
        movable = [i for i in range(1, number_of) if counts[i] < largest] or [i for i in range(1, number_of) if counts[i] < limit]
        mass, budget = sum([portions[i] for i in movable]), rest
        for i in movable:
            addition = min(limit - counts[i], max(1, budget * portions[i] // mass), rest)
            counts[i] = counts[i] + addition
            rest = rest - addition
    return np.array(counts)


def bell_draw(rng, dims, spread, reach, pieces=(), held_as=jnp.bfloat16):
    entries = jax.random.normal(rng, dims, jnp.float32) * spread
    if len(pieces) > 0:
        entries = shard_levels(rng, dims, pieces, -0.22, 0.18) * entries
    return jnp.clip(entries, min=-reach, max=reach).astype(held_as)


def setup_inputs(seed: int = 0) -> dict:
    keys = jax.random.split(jax.random.key(seed), 8)
    tokens = bell_draw(keys[0], (TOKENS, D), 1.0, 6.0, ((0, 8),))
    norm_gain = jnp.clip(1.0 + 0.18 * jax.random.normal(keys[1], (D,), jnp.float32), 0.1, 1.9)
    gate_train = bell_draw(keys[2], (EXPERTS, D, FF), D ** -0.5, 0.125, ((1, 8), (2, 4)), jnp.float32)
    up_train = bell_draw(keys[3], (EXPERTS, D, FF), D ** -0.5, 0.125, ((1, 8), (2, 4)), jnp.float32)
    down_train = bell_draw(keys[4], (EXPERTS, FF, D), FF ** -0.5, 0.21875, ((1, 8), (2, 4)), jnp.float32)
    expert_ids_keys = jax.random.split(jax.random.fold_in(keys[5], 1), TOKENS // TOK_DEV)
    expert_ids_turns = jax.random.permutation(jax.random.fold_in(keys[5], 3), TOKENS // TOK_DEV)
    expert_ids = jax.vmap(lambda own, number: shared_out(jax.random.fold_in(keys[5], 2), own, number, TOK_DEV, EXPERTS, TOP, CAP, 2))(expert_ids_keys, expert_ids_turns).reshape((TOKENS, TOP))
    route_weights = jnp.clip(jnp.exp(math.log(1.0) - 2.3025851 * jax.random.uniform(keys[6], (TOKENS, TOP), jnp.float32) ** shard_levels(keys[6], (TOKENS, TOP), ((0, 8),), -0.2, 0.2)), 0.1, 1.0)
    return dict(tokens=tokens, norm_gain=norm_gain, gate_train=gate_train, up_train=up_train, down_train=down_train, expert_ids=expert_ids, route_weights=route_weights)


epsilon = 1e-06

def reference(tokens, norm_gain, gate_train, up_train, down_train, expert_ids, route_weights):
    gate_serve = (norm_gain[None, :, None] * gate_train).astype(jnp.bfloat16)
    up_serve = (norm_gain[None, :, None] * up_train).astype(jnp.bfloat16)
    down_serve = down_train.astype(jnp.bfloat16)
    tok_float = tokens.astype(jnp.float32)
    normed = (tok_float * lax.rsqrt(lax.optimization_barrier(jnp.mean(tok_float * tok_float, axis=-1, keepdims=True)) + epsilon)).astype(jnp.bfloat16)
    flat_ids = expert_ids.reshape(N_FS, TOK_DEV * TOP)
    onehot = (flat_ids[:, :, None] == jnp.arange(EXPERTS, dtype=jnp.int32)[None, None, :]).astype(jnp.int32)
    slot_rank = lax.optimization_barrier(jnp.sum((jnp.cumsum(onehot, axis=1) - onehot) * onehot, axis=-1))
    row_index = (jnp.arange(N_FS, dtype=jnp.int32)[:, None] * CAP + slot_rank).astype(jnp.int32)
    tok_index = (jnp.arange(N_FS, dtype=jnp.int32)[:, None] * TOK_DEV + jnp.arange(TOK_DEV * TOP, dtype=jnp.int32)[None, :] // TOP).astype(jnp.int32)
    buffer = jnp.zeros((EXPERTS, N_FS * CAP, D), jnp.bfloat16)
    buffer = buffer.at[flat_ids.reshape(-1), row_index.reshape(-1)].set(normed[tok_index.reshape(-1)])
    block_width = FF // N_TP

    def expert_apply(inputs):
        routed, weight_gate, weight_up, weight_down = inputs
        gate_act = jnp.dot(routed, weight_gate, preferred_element_type=jnp.float32)
        up_act = jnp.dot(routed, weight_up, preferred_element_type=jnp.float32)
        hidden = (jax.nn.silu(gate_act) * up_act).astype(jnp.bfloat16)
        running = jnp.zeros((routed.shape[0], D), jnp.float32)
        for index_tp in range(N_TP):
            partial_value = jnp.dot(hidden[:, index_tp * block_width:(index_tp + 1) * block_width], weight_down[index_tp * block_width:(index_tp + 1) * block_width], preferred_element_type=jnp.float32)
            running = running + partial_value.astype(jnp.bfloat16).astype(jnp.float32)
        return running.astype(jnp.bfloat16)
    outputs = lax.map(expert_apply, (buffer, gate_serve, up_serve, down_serve))
    picked = outputs[flat_ids.reshape(-1), row_index.reshape(-1)].reshape(TOKENS, TOP, D).astype(jnp.float32)
    shares = route_weights / lax.optimization_barrier(jnp.sum(route_weights, axis=-1, keepdims=True))
    mixed = lax.optimization_barrier(jnp.sum(shares[:, :, None] * picked, axis=1)).astype(jnp.bfloat16)
    return (gate_serve, up_serve, down_serve, mixed)
```

```python
import functools

import jax
import jax.numpy as jnp
from jax import lax
from jax.experimental import pallas as pl
from jax.experimental.pallas import tpu as pltpu
from jax.sharding import PartitionSpec as P

epsilon = 1e-06


def gathered(tokens, norm_gain, gate_train, up_train, down_train, expert_ids, route_weights):
    experts, rows, cols = gate_train.shape
    fs_at = lax.axis_index("fs")
    tok_rows, picks = expert_ids.shape
    down_rows, down_cols = down_train.shape[1:]
    fs_count = lax.axis_size("fs")

    gate_up = jnp.concatenate(
        [norm_gain[None, :, None] * gate_train, norm_gain[None, :, None] * up_train], axis=2
    ).astype(jnp.bfloat16)
    gate_up = gate_up.transpose(1, 0, 2).reshape(rows, experts * 2 * cols)
    gate_up_all = lax.all_gather(gate_up, "fs", axis=0, tiled=True)
    down_all = lax.all_gather(
        down_train.astype(jnp.bfloat16).reshape(experts * down_rows, down_cols),
        "fs", axis=0, tiled=True,
    )

    tok_float = tokens.astype(jnp.float32)
    normed = (
        tok_float * lax.rsqrt(jnp.mean(tok_float * tok_float, axis=-1, keepdims=True) + epsilon)
    ).astype(jnp.bfloat16)
    shares = route_weights / jnp.sum(route_weights, axis=-1, keepdims=True)

    group = 2 * lax.axis_size("tp")
    picked = [jnp.zeros((tok_rows, cols), jnp.float32) for _ in range(picks)]
    for first in range(0, experts, group):
        part = gate_up_all[:, first * 2 * cols : (first + group) * 2 * cols]
        if first:
            part, picked = lax.optimization_barrier((part, picked))
        acts = jnp.dot(normed, part, preferred_element_type=jnp.float32)
        for at in range(group):
            g = acts[:, at * 2 * cols : at * 2 * cols + cols]
            u = acts[:, at * 2 * cols + cols : (at + 1) * 2 * cols]
            h = jax.nn.silu(g) * u
            for k in range(picks):
                picked[k] = picked[k] + jnp.where(
                    expert_ids[:, k : k + 1] == first + at, h, 0.0
                )
    hidden = jnp.stack([picked[k] * shares[:, k : k + 1] for k in range(picks)], 0)
    hidden_all = lax.all_gather(hidden.astype(jnp.bfloat16), "tp", axis=2, tiled=True)
    hidden_all = hidden_all.reshape(picks, tok_rows, fs_count, 1, down_rows)
    ids = jnp.arange(experts, dtype=jnp.int32)[None, None, :, None]
    mixed = jnp.zeros((tok_rows, down_cols), jnp.float32)
    for first in range(0, fs_count, group):
        blocks = hidden_all[:, :, first : first + group]
        if first:
            blocks, mixed = lax.optimization_barrier((blocks, mixed))
        spread = jnp.zeros((tok_rows, group, experts, down_rows), jnp.bfloat16)
        for k in range(picks):
            spread = jnp.where(expert_ids[:, k][:, None, None, None] == ids, blocks[k], spread)
        depth = experts * down_rows
        mixed = mixed + jnp.dot(
            spread.reshape(tok_rows, group * depth),
            down_all[first * depth : (first + group) * depth],
            preferred_element_type=jnp.float32,
        )
    mixed = mixed.astype(jnp.bfloat16)

    own = lax.dynamic_slice_in_dim(gate_up_all, fs_at * 2 * cols, 2 * cols, 1)
    down_own = lax.dynamic_slice_in_dim(
        down_all.reshape(fs_count, experts, down_rows, down_cols), fs_at, 1, 1
    ).reshape(1, fs_count * down_rows, down_cols)
    down_serve = lax.all_to_all(down_own, "tp", split_axis=1, concat_axis=2, tiled=True)
    return own[None, :, :cols], own[None, :, cols:], down_serve, mixed


def ladder_kernel(
    n, tp_count, parts, ahead, blocks, gu_ref, dn_ref, tokens_ref, meta_ref,
    serve_g, serve_u, serve_d, mixed_ref,
    gu_all, dn_all, far_tokens, far_meta, cols, fold, picks, total, reply, answer,
    send_sem, recv_sem, tok_send, tok_recv, meta_send, meta_recv,
    pick_send, pick_recv, reply_send, reply_recv, serve_send, serve_recv,
):
    fs_at, tp_at = lax.axis_index("fs"), lax.axis_index("tp")
    rows = gu_ref.shape[1]
    width = gu_ref.shape[2]
    down_rows, down_cols = dn_ref.shape[2:]
    tok_rows = tokens_ref.shape[0]
    height = tok_rows // blocks
    quarter = n // 4
    base = (quarter, 2 * quarter, 0, 3 * quarter)
    gates = 4 * parts
    units = 6 * parts
    chunk = rows // parts

    z, y = fs_at // 2, fs_at % 2
    side = z // 2
    mid = jnp.logical_or(z == 1, z == 2)
    end = jnp.logical_not(mid)
    near_mid, far_mid = 1 + side, 2 - side
    near_end, far_end = 3 * side, 3 - 3 * side

    def at(zz, yy):
        return zz * 2 + yy

    E, Eo = at(near_end, y), at(near_end, 1 - y)
    M, R = at(near_mid, y), at(near_mid, 1 - y)
    X, Xo = at(far_mid, y), at(far_mid, 1 - y)
    F, Fo = at(far_end, y), at(far_end, 1 - y)
    across = tp_at + 2 - 4 * (tp_at // 2)
    mate = tp_at + 1 - 2 * (tp_at % 2)
    diagonal = across + 1 - 2 * (tp_at % 2)

    MESH = pl.DeviceIdType.MESH
    barrier = pltpu.get_barrier_semaphore()

    def greet(to):
        pl.semaphore_signal(barrier, inc=1, device_id=to, device_id_type=MESH)

    for hop in range(1, tp_count):
        greet({"tp": (tp_at + hop) % tp_count})

    @pl.when(mid)
    def _():
        greet({"fs": E})
        greet({"fs": R})
        greet({"fs": X})
        pl.semaphore_wait(barrier, tp_count + 2)

    @pl.when(end)
    def _():
        greet({"fs": M})
        greet({"fs": Eo})
        pl.semaphore_wait(barrier, tp_count + 1)

    def gu_view(u, s):
        return gu_all.at[u // parts, pl.ds(pl.multiple_of(s * rows + (u % parts) * chunk, chunk), chunk), :]

    def gu_own(u):
        return gu_ref.at[u // parts, pl.ds(pl.multiple_of((u % parts) * chunk, chunk), chunk), :]

    def dn_view(u, s):
        v = u - gates
        span = pl.ds(pl.multiple_of((s % 2) * down_rows, down_rows), down_rows)
        if parts == 4:
            return dn_all.at[v // 2, s // 2, v % 2, span, :]
        return dn_all.at[v, s // 2, :, span, :]

    def dn_own(u):
        v = u - gates
        return dn_ref.at[v // 2, v % 2] if parts == 4 else dn_ref.at[v]

    def copy(view, u, s, to, slot, src=None):
        place = view(u, s)
        return pltpu.make_async_remote_copy(
            src_ref=place if src is None else src, dst_ref=place,
            send_sem=send_sem.at[slot, u], recv_sem=recv_sem.at[s, u],
            device_id={"fs": to}, device_id_type=MESH,
        )

    def group(u, body):
        @pl.when(jnp.logical_and(u >= 0, u < gates))
        def _():
            body(u, gu_view, gu_own, u >= 2 * parts)

        @pl.when(jnp.logical_and(u >= gates, u < units))
        def _():
            body(u, dn_view, dn_own, u >= 5 * parts)

    def sends(u):
        def from_mid(u, view, own, wide):
            copy(view, u, fs_at, R, 0, own(u)).start()
            copy(view, u, fs_at, X, 3, own(u)).start()
            pl.when(wide)(lambda: copy(view, u, fs_at, E, 6, own(u)).start())

        def from_end(u, view, own, wide):
            copy(view, u, fs_at, M, 0, own(u)).start()
            copy(view, u, fs_at, Eo, 2, own(u)).start()

        pl.when(mid)(lambda: group(u, from_mid))
        pl.when(end)(lambda: group(u, from_end))

    def got(view, u, s):
        copy(view, u, s, s, 0).wait_recv()

    token_parts = 2 * parts
    token_rows = tok_rows // tp_count // token_parts
    token_from = 1

    def token_copy(j, owner, kind, to):
        span = pl.ds(pl.multiple_of((owner * token_parts + j) * token_rows, token_rows), token_rows)
        return pltpu.make_async_remote_copy(
            src_ref=tokens_ref.at[span] if kind == 0 else far_tokens.at[span],
            dst_ref=far_tokens.at[span],
            send_sem=tok_send.at[max(kind - 1, 0), j], recv_sem=tok_recv.at[owner, j],
            device_id=to, device_id_type=MESH,
        )

    def tick(t):
        sends(t + ahead)

        @pl.when(mid)
        def _():
            def first(u, view, own, wide):
                got(view, u, E)
                copy(view, u, E, X, 4).start()
                got(view, u, X)
                copy(view, u, X, R, 1).start()
                pl.when(wide)(lambda: copy(view, u, X, E, 7).start())
                got(view, u, R)

            def second(u, view, own, wide):
                got(view, u, Eo)
                pl.when(u % 2 == 1)(lambda: copy(view, u, Eo, X, 5).start())
                got(view, u, F)
                pl.when(u % 2 == 0)(lambda: copy(view, u, F, R, 2).start())
                pl.when(wide)(lambda: copy(view, u, F, E, 8).start())
                got(view, u, Xo)

            group(t, first)
            group(t - 1, second)
            group(t - 2, lambda u, view, own, wide: got(view, u, Fo))
            j = t - token_from - 1

            @pl.when(jnp.logical_and(j >= 0, j < token_parts))
            def _():
                token_copy(j, tp_at, 1, {"tp": across}).wait_recv()
                token_copy(j, tp_at, 1, {"tp": across}).start()
                token_copy(j, tp_at, 2, {"tp": mate}).start()

            i = j - 1

            @pl.when(jnp.logical_and(i >= 0, i < token_parts))
            def _():
                token_copy(i, across, 3, {"tp": mate}).wait_recv()
                token_copy(i, across, 3, {"tp": mate}).start()

        @pl.when(end)
        def _():
            def first(u, view, own, wide):
                got(view, u, Eo)
                copy(view, u, Eo, M, 1).start()

                @pl.when(wide)
                def _():
                    got(view, u, M)
                    copy(view, u, M, Eo, 3).start()

            def second(u, view, own, wide):
                @pl.when(wide)
                def _():
                    got(view, u, X)
                    copy(view, u, X, Eo, 4).start()
                    got(view, u, R)

            def third(u, view, own, wide):
                @pl.when(wide)
                def _():
                    got(view, u, F)
                    copy(view, u, F, Eo, 5).start()
                    got(view, u, Xo)

            def fourth(u, view, own, wide):
                pl.when(wide)(lambda: got(view, u, Fo))

            group(t, first)
            group(t - 1, second)
            group(t - 2, third)
            group(t - 3, fourth)
            j = t - token_from

            @pl.when(jnp.logical_and(j >= 0, j < token_parts))
            def _():
                token_copy(j, tp_at, 0, {"fs": M}).start()

    meta_copy = pltpu.make_async_remote_copy(
        src_ref=meta_ref, dst_ref=far_meta, send_sem=meta_send, recv_sem=meta_recv,
        device_id={"fs": M}, device_id_type=MESH,
    )

    def loop(first, last, body):
        def step(t, carry):
            body(t)
            return carry

        lax.fori_loop(first, last, step, 0)

    loop(0, ahead, sends)
    pl.when(end)(meta_copy.start)
    gu_all[:, pl.ds(pl.multiple_of(fs_at * rows, rows), rows), :] = gu_ref[...]
    dn_all[:, fs_at // 2, :, pl.ds(pl.multiple_of((fs_at % 2) * down_rows, down_rows), down_rows), :] = dn_ref[...]

    def columns(which, ref):
        for b in range(tok_rows // 128):
            cols[which, pl.ds(b * 128, 128), :] = jnp.transpose(ref[:, pl.ds(b * 128, 128)])

    columns(0, meta_ref)

    lane = lax.broadcasted_iota(jnp.int32, (1, 384), 1)
    parity = jnp.where(lane < 256, lane // 128, (lane - 256) // 64).astype(jnp.float32)
    low = lax.broadcasted_iota(jnp.int32, (1, 128), 1) < 64

    def span_of(block):
        return pl.ds(pl.multiple_of(block * height, height), height)

    def evaluate(block, ref, which, phase):
        span = span_of(block)
        tokens = ref[span, :].astype(jnp.float32)
        square = jnp.mean(tokens * tokens, axis=-1, keepdims=True)
        tokens = (tokens * lax.rsqrt(square + epsilon)).astype(jnp.bfloat16)
        ids = [cols[which, span, pl.ds(k, 1)] for k in (0, 1)]
        gate = jnp.dot(tokens, gu_all[2 * phase], preferred_element_type=jnp.float32)
        up = jnp.dot(tokens, gu_all[2 * phase + 1], preferred_element_type=jnp.float32)
        hidden = gate / (1.0 + jnp.exp(-gate)) * up
        folded = []
        for k in (0, 1):
            value = jnp.zeros((height, 384), jnp.float32)
            for pair in (0, 1):
                named = base[2 * phase + pair] + parity
                part = hidden[:, pair * 384 : (pair + 1) * 384]
                value = value + jnp.where(ids[k] == named, part, 0.0)
            folded.append(value)
        return folded

    def pick_copy(block, which, owner, kind, to):
        place = picks.at[which, owner, span_of(block), :]
        return pltpu.make_async_remote_copy(
            src_ref=place, dst_ref=place,
            send_sem=pick_send.at[which, kind, block], recv_sem=pick_recv.at[which, owner, block],
            device_id={"tp": to}, device_id_type=MESH,
        )

    def share(block, which, folded):
        span = span_of(block)
        routes = [cols[which, span, pl.ds(2 + k, 1)] for k in (0, 1)]
        folded = [folded[k] * (routes[k] / (routes[0] + routes[1])) for k in (0, 1)]
        ends = [f[:, 256:384] + pltpu.roll(f[:, 256:384], 64, 1) for f in folded]
        for k in (0, 1):
            whole = folded[k][:, :128] + folded[k][:, 128:256]
            picks[which, tp_at, span, pl.ds(k * 128, 128)] = whole.astype(jnp.bfloat16)
        picks[which, tp_at, span, pl.ds(256, 128)] = jnp.where(low, ends[0], ends[1]).astype(
            jnp.bfloat16
        )
        pick_copy(block, which, tp_at, 0, across).start()
        pick_copy(block, which, tp_at, 1, mate).start()

    def pass_on(block, which):
        pick_copy(block, which, across, 2, mate).wait_recv()
        pick_copy(block, which, across, 2, mate).start()

    def picked_up(block, which):
        pick_copy(block, which, mate, 0, mate).wait_recv()
        pick_copy(block, which, diagonal, 0, mate).wait_recv()

    def project(block, which, phase):
        span = span_of(block)
        ids = [cols[which, span, pl.ds(k, 1)] for k in (0, 1)]
        product = None
        for index in range(tp_count):
            held = picks[which, index, span, :].astype(jnp.float32)
            tail = held[:, 256:384]
            turned = pltpu.roll(tail, 64, 1)
            ends = [jnp.where(low, tail, turned), jnp.where(low, turned, tail)]
            pieces, weights = [], []
            for pair in (2 * phase, 2 * phase + 1):
                for e in (0, 1):
                    named = float(base[pair] + e)
                    pieces.append(
                        jnp.where(ids[0] == named, held[:, :128],
                                  jnp.where(ids[1] == named, held[:, 128:256], 0.0))
                    )
                    weights.append(dn_all[pair, index, e, pl.ds(0, 128), :])
                named = base[pair] + parity[:, 256:384]
                pieces.append(
                    jnp.where(ids[0] == named, ends[0], jnp.where(ids[1] == named, ends[1], 0.0))
                )
                for e in (0, 1):
                    weights.append(dn_all[pair, index, e, pl.ds(128, 64), :])
            spread = jnp.concatenate([p.astype(jnp.bfloat16) for p in pieces], axis=1)
            part = jnp.dot(
                spread, jnp.concatenate(weights, axis=0), preferred_element_type=jnp.float32
            )
            product = part if product is None else product + part
        return product

    def reply_copy(block):
        return pltpu.make_async_remote_copy(
            src_ref=reply.at[span_of(block)], dst_ref=answer.at[span_of(block)],
            send_sem=reply_send.at[block], recv_sem=reply_recv.at[block],
            device_id={"fs": E}, device_id_type=MESH,
        )

    start = 2 * parts + 2
    loop(0, start, tick)

    @pl.when(end)
    def _():
        fold[...] = jnp.zeros_like(fold)

    @pl.when(mid)
    def _():
        meta_copy.wait_recv()
        columns(1, far_meta)

    def own_first(t):
        tick(t)

        @pl.when(mid)
        def _():
            folded = evaluate(t - start, tokens_ref, 0, 0)
            span = span_of(t - start)
            for k in (0, 1):
                fold[k, span, :] = folded[k]

    loop(start, start + blocks, own_first)
    start = start + blocks

    @pl.when(mid)
    def _():
        def landed(j):
            token_copy(j, mate, 1, {"tp": mate}).wait_recv()
            token_copy(j, diagonal, 1, {"tp": mate}).wait_recv()

        loop(0, token_parts, landed)

    def far_first(t):
        tick(t)

        @pl.when(mid)
        def _():
            share(t - start, 1, evaluate(t - start, far_tokens, 1, 0))

    loop(start, start + blocks, far_first)
    start = start + blocks
    ready = max(start, gates + 3)
    loop(start, ready, tick)
    start = ready

    def served(part):
        span = pl.ds(pl.multiple_of(part * rows, rows), rows)
        phase = jnp.where(mid, 0, 1)
        for kind, out in ((0, serve_g), (1, serve_u)):
            out[span, pl.ds(0, 128)] = gu_all[
                2 * phase + kind, span, pl.ds(pl.multiple_of(side * 384 + y * 128, 128), 128)
            ]
            tail = gu_all[
                2 * phase + kind, span, pl.ds(pl.multiple_of(side * 384 + 256, 128), 128)
            ].astype(jnp.float32)
            tail = jnp.where(y == 1, pltpu.roll(tail, 64, 1), tail)
            out[span, pl.ds(128, 64)] = tail[:, :64].astype(jnp.bfloat16)

    def own_second(t):
        tick(t)
        block = t - start
        folded = evaluate(block, tokens_ref, 0, 1)
        span = span_of(block)
        share(block, 0, [folded[k] + fold[k, span, :] for k in (0, 1)])
        pl.when(mid)(lambda: pass_on(block, 1))

    loop(start, start + blocks, own_second)
    start = start + blocks

    def far_second(t):
        tick(t)
        block = t - start
        pass_on(block, 0)

        @pl.when(mid)
        def _():
            picked_up(block, 1)
            reply[span_of(block)] = project(block, 1, 0).astype(jnp.bfloat16)
            reply_copy(block).start()

    loop(start, start + blocks, far_second)
    start = start + blocks
    loop(start, max(start, units + 3), tick)

    pair = jnp.where(mid, side, 2 + side)

    def serve_copy(to, owner):
        return pltpu.make_async_remote_copy(
            src_ref=dn_all.at[pair, to, y],
            dst_ref=serve_d.at[:, pl.ds(pl.multiple_of(owner * down_cols, down_cols), down_cols)],
            send_sem=serve_send.at[to], recv_sem=serve_recv.at[owner],
            device_id={"tp": to}, device_id_type=MESH,
        )

    for hop in range(1, tp_count):
        serve_copy((tp_at + hop) % tp_count, tp_at).start()
    serve_d[:, pl.ds(pl.multiple_of(tp_at * down_cols, down_cols), down_cols)] = dn_all[pair, tp_at, y]
    loop(0, n, served)

    def finish(block):
        span = span_of(block)
        picked_up(block, 0)

        @pl.when(mid)
        def _():
            total[span, :] = project(block, 0, 0)

        @pl.when(end)
        def _():
            reply_copy(block).wait_recv()
            total[span, :] = answer[span, :].astype(jnp.float32)

        mixed_ref[span, :] = (total[span, :] + project(block, 0, 1)).astype(jnp.bfloat16)

    loop(0, blocks, finish)

    def drained(u):
        def from_mid(u, view, own, wide):
            for slot in (0, 1, 3, 4):
                copy(view, u, fs_at, X, slot).wait_send()
            pl.when(u % 2 == 0)(lambda: copy(view, u, fs_at, X, 2).wait_send())
            pl.when(u % 2 == 1)(lambda: copy(view, u, fs_at, X, 5).wait_send())

            @pl.when(wide)
            def _():
                for slot in (6, 7, 8):
                    copy(view, u, fs_at, X, slot).wait_send()

        def from_end(u, view, own, wide):
            for slot in (0, 1, 2):
                copy(view, u, fs_at, M, slot).wait_send()

            @pl.when(wide)
            def _():
                for slot in (3, 4, 5):
                    copy(view, u, fs_at, M, slot).wait_send()

        pl.when(mid)(lambda: group(u, from_mid))
        pl.when(end)(lambda: group(u, from_end))

    loop(0, units, drained)

    @pl.when(mid)
    def _():
        def token_drain(j):
            for kind in (1, 2, 3):
                token_copy(j, tp_at, kind, {"tp": mate}).wait_send()

        loop(0, token_parts, token_drain)

        def block_drain(b):
            reply_copy(b).wait_send()
            for kind in (0, 1, 2):
                pick_copy(b, 1, tp_at, kind, mate).wait_send()

        loop(0, blocks, block_drain)

    @pl.when(end)
    def _():
        meta_copy.wait_send()
        loop(0, token_parts, lambda j: token_copy(j, tp_at, 0, {"fs": M}).wait_send())

    def own_drain(b):
        for kind in (0, 1, 2):
            pick_copy(b, 0, tp_at, kind, mate).wait_send()

    loop(0, blocks, own_drain)
    for hop in range(1, tp_count):
        to = (tp_at + hop) % tp_count
        serve_copy(to, tp_at).wait_send()
        serve_copy(tp_at, to).wait_recv()


def laddered(tokens, norm_gain, gate_train, up_train, down_train, expert_ids, route_weights):
    experts, rows, cols = gate_train.shape
    down_rows, down_cols = down_train.shape[1:]
    n, tp_count = lax.axis_size("fs"), lax.axis_size("tp")
    tok_rows, width = tokens.shape
    half, quarter = experts // 2, experts // 4
    blocks, parts, ahead = 4, 4, 3

    def paired(train):
        value = (norm_gain[None, :, None] * train).astype(jnp.bfloat16)
        value = jnp.concatenate([value[quarter:-quarter], value[:quarter], value[-quarter:]], axis=0)
        value = value.transpose(1, 0, 2).reshape(rows, 2, 2, 2, cols)
        value = jnp.concatenate(
            [value[..., :128].reshape(rows, 2, 2, 256), value[..., 128:].reshape(rows, 2, 2, 128)],
            axis=3,
        )
        return value.transpose(1, 0, 2, 3).reshape(2, rows, 768)

    gate, up = paired(gate_train), paired(up_train)
    gu = jnp.stack([gate, up], axis=1).reshape(4, rows, 768)
    down = down_train.astype(jnp.bfloat16)
    down = jnp.concatenate([down[quarter:-quarter], down[:quarter], down[-quarter:]], axis=0)
    down = down.reshape(4, 2, down_rows, down_cols)
    meta = jnp.concatenate(
        [expert_ids.T.astype(jnp.float32), route_weights.T, jnp.zeros((4, tok_rows), jnp.float32)],
        axis=0,
    )
    vmem = pl.BlockSpec(memory_space=pltpu.VMEM)
    dma = pltpu.SemaphoreType.DMA
    bf16, f32 = jnp.bfloat16, jnp.float32
    units = 6 * parts
    gate_serve, up_serve, down_serve, mixed = pl.pallas_call(
        functools.partial(ladder_kernel, n, tp_count, parts, ahead, blocks),
        out_shape=(
            jax.ShapeDtypeStruct((width, cols), bf16),
            jax.ShapeDtypeStruct((width, cols), bf16),
            jax.ShapeDtypeStruct((2 * down_rows, width), bf16),
            jax.ShapeDtypeStruct((tok_rows, down_cols), bf16),
        ),
        in_specs=[vmem] * 4,
        out_specs=(vmem,) * 4,
        scratch_shapes=[
            pltpu.VMEM((4, width, 768), bf16),
            pltpu.VMEM((4, tp_count, 2, 2 * down_rows, down_cols), bf16),
            pltpu.VMEM((tok_rows, width), bf16),
            pltpu.VMEM((8, tok_rows), f32),
            pltpu.VMEM((2, tok_rows, 8), f32),
            pltpu.VMEM((2, tok_rows, 384), f32),
            pltpu.VMEM((2, tp_count, tok_rows, 384), bf16),
            pltpu.VMEM((tok_rows, down_cols), f32),
            pltpu.VMEM((tok_rows, down_cols), bf16),
            pltpu.VMEM((tok_rows, down_cols), bf16),
            dma((9, units)),
            dma((n, units)),
            dma((3, 2 * parts)),
            dma((tp_count, 2 * parts)),
            dma,
            dma,
            dma((2, 3, blocks)),
            dma((2, tp_count, blocks)),
            dma((blocks,)),
            dma((blocks,)),
            dma((tp_count,)),
            dma((tp_count,)),
        ],
        compiler_params=pltpu.CompilerParams(
            collective_id=0, has_side_effects=True, vmem_limit_bytes=63 * 1024 * 1024
        ),
    )(gu, down, tokens, meta)
    return gate_serve[None], up_serve[None], down_serve[None], mixed


def on_device(tokens, norm_gain, gate_train, up_train, down_train, expert_ids, route_weights):
    experts, rows, cols = gate_train.shape
    n, tp_count = lax.axis_size("fs"), lax.axis_size("tp")
    fits = experts == n and n == 2 * tp_count and cols == 192 and expert_ids.shape[1] == 2
    held = 3 * experts * n * rows * cols * 2
    run = laddered if fits and held < 24 * 1024 * 1024 else gathered
    return run(
        tokens, norm_gain, gate_train, up_train, down_train, expert_ids, route_weights
    )


def solution(mesh):
    return jax.shard_map(
        on_device,
        mesh=mesh,
        in_specs=(
            P("fs", None),
            P("fs"),
            P(None, "fs", "tp"),
            P(None, "fs", "tp"),
            P(None, "fs", "tp"),
            P("fs", None),
            P("fs", None),
        ),
        out_specs=(P("fs", None, "tp"), P("fs", None, "tp"), P("fs", "tp", None), P("fs", "tp")),
        check_vma=False,
    )
```

```python
import functools

import jax
import jax.numpy as jnp
from jax import lax
from jax.experimental import pallas as pl
from jax.experimental.pallas import tpu as pltpu
from jax.sharding import PartitionSpec as P

epsilon = 1e-06


def gathered(tokens, norm_gain, gate_train, up_train, down_train, expert_ids, route_weights):
    experts, rows, cols = gate_train.shape
    fs_at = lax.axis_index("fs")
    tok_rows, picks = expert_ids.shape
    down_rows, down_cols = down_train.shape[1:]
    fs_count = lax.axis_size("fs")

    gate_up = jnp.concatenate(
        [norm_gain[None, :, None] * gate_train, norm_gain[None, :, None] * up_train], axis=2
    ).astype(jnp.bfloat16)
    gate_up = gate_up.transpose(1, 0, 2).reshape(rows, experts * 2 * cols)
    gate_up_all = lax.all_gather(gate_up, "fs", axis=0, tiled=True)
    down_all = lax.all_gather(
        down_train.astype(jnp.bfloat16).reshape(experts * down_rows, down_cols),
        "fs", axis=0, tiled=True,
    )

    tok_float = tokens.astype(jnp.float32)
    normed = (
        tok_float * lax.rsqrt(jnp.mean(tok_float * tok_float, axis=-1, keepdims=True) + epsilon)
    ).astype(jnp.bfloat16)
    shares = route_weights / jnp.sum(route_weights, axis=-1, keepdims=True)

    group = 2 * lax.axis_size("tp")
    picked = [jnp.zeros((tok_rows, cols), jnp.float32) for _ in range(picks)]
    for first in range(0, experts, group):
        part = gate_up_all[:, first * 2 * cols : (first + group) * 2 * cols]
        if first:
            part, picked = lax.optimization_barrier((part, picked))
        acts = jnp.dot(normed, part, preferred_element_type=jnp.float32)
        for at in range(group):
            g = acts[:, at * 2 * cols : at * 2 * cols + cols]
            u = acts[:, at * 2 * cols + cols : (at + 1) * 2 * cols]
            h = jax.nn.silu(g) * u
            for k in range(picks):
                picked[k] = picked[k] + jnp.where(
                    expert_ids[:, k : k + 1] == first + at, h, 0.0
                )
    hidden = jnp.stack([picked[k] * shares[:, k : k + 1] for k in range(picks)], 0)
    hidden_all = lax.all_gather(hidden.astype(jnp.bfloat16), "tp", axis=2, tiled=True)
    hidden_all = hidden_all.reshape(picks, tok_rows, fs_count, 1, down_rows)
    ids = jnp.arange(experts, dtype=jnp.int32)[None, None, :, None]
    mixed = jnp.zeros((tok_rows, down_cols), jnp.float32)
    for first in range(0, fs_count, group):
        blocks = hidden_all[:, :, first : first + group]
        if first:
            blocks, mixed = lax.optimization_barrier((blocks, mixed))
        spread = jnp.zeros((tok_rows, group, experts, down_rows), jnp.bfloat16)
        for k in range(picks):
            spread = jnp.where(expert_ids[:, k][:, None, None, None] == ids, blocks[k], spread)
        depth = experts * down_rows
        mixed = mixed + jnp.dot(
            spread.reshape(tok_rows, group * depth),
            down_all[first * depth : (first + group) * depth],
            preferred_element_type=jnp.float32,
        )
    mixed = mixed.astype(jnp.bfloat16)

    own = lax.dynamic_slice_in_dim(gate_up_all, fs_at * 2 * cols, 2 * cols, 1)
    down_own = lax.dynamic_slice_in_dim(
        down_all.reshape(fs_count, experts, down_rows, down_cols), fs_at, 1, 1
    ).reshape(1, fs_count * down_rows, down_cols)
    down_serve = lax.all_to_all(down_own, "tp", split_axis=1, concat_axis=2, tiled=True)
    return own[None, :, :cols], own[None, :, cols:], down_serve, mixed


def ladder_kernel(
    n, tp_count, parts, ahead, lag, blocks, gate_in, up_in, down_in, gain_ref, tokens_in, ids_ref,
    routes_ref, serve_g, serve_u, serve_d, mixed_ref,
    gate_stage, up_stage, down_stage, tokens_ref, meta_ref, stage_sem, gu_all, dn_all, far_tokens, far_meta, cols, fold, picks, total, reply, answer,
    send_sem, recv_sem, tok_send, tok_recv, meta_send, meta_recv,
    pick_send, pick_recv, reply_send, reply_recv, serve_send, serve_recv,
):
    fs_at, tp_at = lax.axis_index("fs"), lax.axis_index("tp")
    rows = gate_in.shape[2]
    down_rows, down_cols = down_in.shape[1:]
    tok_rows = tokens_in.shape[0]
    height = tok_rows // blocks
    quarter = n // 4
    base = (quarter, 2 * quarter, 0, 3 * quarter)
    gates = 4 * parts
    units = 6 * parts
    chunk = gu_all.shape[1] // parts

    z, y = fs_at // 2, fs_at % 2
    side = z // 2
    mid = jnp.logical_or(z == 1, z == 2)
    end = jnp.logical_not(mid)
    near_mid, far_mid = 1 + side, 2 - side
    near_end, far_end = 3 * side, 3 - 3 * side

    def at(zz, yy):
        return zz * 2 + yy

    E, Eo = at(near_end, y), at(near_end, 1 - y)
    M, R = at(near_mid, y), at(near_mid, 1 - y)
    X, Xo = at(far_mid, y), at(far_mid, 1 - y)
    F, Fo = at(far_end, y), at(far_end, 1 - y)
    across = tp_at + 2 - 4 * (tp_at // 2)
    mate = tp_at + 1 - 2 * (tp_at % 2)
    diagonal = across + 1 - 2 * (tp_at % 2)

    stages = [
        pltpu.make_async_copy(src, dst, stage_sem.at[k])
        for k, (src, dst) in enumerate(
            [(gate_in, gate_stage), (up_in, up_stage), (down_in, down_stage), (tokens_in, tokens_ref)]
        )
    ]
    for stage in stages:
        stage.start()

    MESH = pl.DeviceIdType.MESH
    barrier = pltpu.get_barrier_semaphore()

    def greet(to):
        pl.semaphore_signal(barrier, inc=1, device_id=to, device_id_type=MESH)

    for hop in range(1, tp_count):
        greet({"tp": (tp_at + hop) % tp_count})

    @pl.when(mid)
    def _():
        greet({"fs": E})
        greet({"fs": R})
        greet({"fs": X})

    @pl.when(end)
    def _():
        greet({"fs": M})
        greet({"fs": Eo})

    own_cols = pl.ds(pl.multiple_of(fs_at * rows, rows), rows)
    own_rows = pl.ds(pl.multiple_of((fs_at % 2) * down_rows, down_rows), down_rows)
    for kind, stage in ((0, gate_stage), (1, up_stage)):
        stages[kind].wait()
        for p in range(4):
            for i in (0, 1):
                value = (stage[base[p] + i] * gain_ref[...]).astype(jnp.bfloat16)
                top = (p % 2) * 384 + i * 128
                low_at = (p % 2) * 384 + 256 + i * 64
                gu_all[2 * (p // 2) + kind, pl.ds(top, 128), own_cols] = value[:128]
                gu_all[2 * (p // 2) + kind, pl.ds(low_at, 64), own_cols] = value[128:]
    stages[2].wait()
    for p in range(4):
        for i in (0, 1):
            dn_all[p, fs_at // 2, i, own_rows, :] = down_stage[base[p] + i].astype(jnp.bfloat16)
    meta_ref[pl.ds(0, 2), :] = ids_ref[...].astype(jnp.float32)
    meta_ref[pl.ds(2, 2), :] = routes_ref[...]
    meta_ref[pl.ds(4, 4), :] = jnp.zeros((4, tok_rows), jnp.float32)
    pl.semaphore_wait(barrier, jnp.where(mid, tp_count + 2, tp_count + 1))

    def is_down(u):
        turn = jnp.logical_and(u >= 3 * parts, u % 2 == 0)
        return jnp.logical_or(turn, u >= 5 * parts)

    def is_wide(u):
        return jnp.logical_or(jnp.logical_and(u >= parts, u % 2 == 1), u >= 5 * parts)

    def gate_at(u):
        turn = parts * (1 + u % 2) + (u - parts) // 2
        return jnp.where(u < parts, u, jnp.where(u < 3 * parts, turn, (u + 3 * parts) // 2))

    def down_at(u):
        return jnp.where(u < 5 * parts, (u - 3 * parts) // 2, u - 4 * parts)

    def wide_at(w):
        return jnp.where(w < 2 * parts, parts + 1 + 2 * w, 3 * parts + w)

    def gu_view(u, s):
        g = gate_at(u)
        return gu_all.at[
            g // parts,
            pl.ds(pl.multiple_of((g % parts) * chunk, chunk), chunk),
            pl.ds(pl.multiple_of(s * rows, rows), rows),
        ]

    def dn_view(u, s):
        v = down_at(u)
        span = pl.ds(pl.multiple_of((s % 2) * down_rows, down_rows), down_rows)
        if parts == 4:
            return dn_all.at[v // 2, s // 2, v % 2, span, :]
        return dn_all.at[v, s // 2, :, span, :]

    def copy(view, u, s, to, slot):
        place = view(u, s)
        return pltpu.make_async_remote_copy(
            src_ref=place, dst_ref=place,
            send_sem=send_sem.at[slot, u], recv_sem=recv_sem.at[s, u],
            device_id={"fs": to}, device_id_type=MESH,
        )

    def group(u, body):
        inside = jnp.logical_and(u >= 0, u < units)

        @pl.when(jnp.logical_and(inside, jnp.logical_not(is_down(u))))
        def _():
            body(u, gu_view, is_wide(u))

        @pl.when(jnp.logical_and(inside, is_down(u)))
        def _():
            body(u, dn_view, is_wide(u))

    def to_far(u, view, wide):
        copy(view, u, fs_at, R, 0).start()
        copy(view, u, fs_at, X, 3).start()

    def to_end(u, view, wide):
        copy(view, u, fs_at, E, 6).start()

    def to_mid(u, view, wide):
        copy(view, u, fs_at, M, 0).start()

    def to_other(u, view, wide):
        copy(view, u, fs_at, Eo, 2).start()

    def sends(t):
        @pl.when(mid)
        def _():
            group(t + ahead, to_far)
            pl.when(t < units // 2)(lambda: group(wide_at(t), to_end))

        @pl.when(end)
        def _():
            group(t + 2, to_mid)
            group(2 * t + 2, to_other)
            group(2 * t + 3, to_other)

    def opening(u):
        pl.when(mid)(lambda: group(u, to_far))

        @pl.when(jnp.logical_and(end, u < 2))
        def _():
            group(u, to_mid)
            group(u, to_other)

    def got(view, u, s):
        copy(view, u, s, s, 0).wait_recv()

    token_parts = 2 * parts
    token_rows = tok_rows // tp_count // token_parts
    token_from = 3

    def token_copy(j, owner, kind, to):
        span = pl.ds(pl.multiple_of((owner * token_parts + j) * token_rows, token_rows), token_rows)
        return pltpu.make_async_remote_copy(
            src_ref=tokens_ref.at[span] if kind == 0 else far_tokens.at[span],
            dst_ref=far_tokens.at[span],
            send_sem=tok_send.at[max(kind - 1, 0), j], recv_sem=tok_recv.at[owner, j],
            device_id=to, device_id_type=MESH,
        )

    def tick(t):
        sends(t)

        @pl.when(mid)
        def _():
            def first(u, view, wide):
                got(view, u, E)
                copy(view, u, E, X, 4).start()
                got(view, u, X)
                copy(view, u, X, R, 1).start()
                pl.when(wide)(lambda: copy(view, u, X, E, 7).start())
                got(view, u, R)

            def second(u, view, wide):
                got(view, u, Eo)
                pl.when(u % 2 == 1)(lambda: copy(view, u, Eo, X, 5).start())
                got(view, u, F)
                pl.when(u % 2 == 0)(lambda: copy(view, u, F, R, 2).start())
                pl.when(wide)(lambda: copy(view, u, F, E, 8).start())
                got(view, u, Xo)

            group(t, first)
            group(t - lag, second)
            group(t - 2 * lag, lambda u, view, wide: got(view, u, Fo))
            j = t - token_from - 2

            @pl.when(jnp.logical_and(j >= 0, j < token_parts))
            def _():
                token_copy(j, tp_at, 1, {"tp": across}).wait_recv()
                token_copy(j, tp_at, 1, {"tp": across}).start()
                token_copy(j, tp_at, 2, {"tp": mate}).start()

            i = j - 1

            @pl.when(jnp.logical_and(i >= 0, i < token_parts))
            def _():
                token_copy(i, across, 3, {"tp": mate}).wait_recv()
                token_copy(i, across, 3, {"tp": mate}).start()

        @pl.when(end)
        def _():
            def first(u, view, wide):
                got(view, u, Eo)
                copy(view, u, Eo, M, 1).start()

            def early(u, view, wide):
                got(view, u, M)
                copy(view, u, M, Eo, 3).start()

            def second(u, view, wide):
                @pl.when(wide)
                def _():
                    got(view, u, X)
                    copy(view, u, X, Eo, 4).start()

            def third(u, view, wide):
                @pl.when(wide)
                def _():
                    got(view, u, F)
                    copy(view, u, F, Eo, 5).start()
                    got(view, u, Xo)

            def fourth(u, view, wide):
                pl.when(wide)(lambda: got(view, u, Fo))

            group(t, first)
            early_at = t - 2 * parts
            pl.when(jnp.logical_and(early_at >= 0, early_at < units // 2))(
                lambda: group(wide_at(early_at), early)
            )
            late_at = early_at - 2
            pl.when(jnp.logical_and(late_at >= 0, late_at < units // 2))(
                lambda: group(wide_at(late_at), lambda u, view, wide: got(view, u, R))
            )
            group(t - lag, second)
            group(t - 2 * lag, third)
            group(t - 3 * lag, fourth)
            j = t - token_from

            @pl.when(jnp.logical_and(j >= 0, j < token_parts))
            def _():
                token_copy(j, tp_at, 0, {"fs": M}).start()

    meta_copy = pltpu.make_async_remote_copy(
        src_ref=meta_ref, dst_ref=far_meta, send_sem=meta_send, recv_sem=meta_recv,
        device_id={"fs": M}, device_id_type=MESH,
    )

    def loop(first, last, body):
        def step(t, carry):
            body(t)
            return carry

        lax.fori_loop(first, last, step, 0)

    loop(0, ahead, opening)
    pl.when(end)(meta_copy.start)

    def columns(which, ref):
        for b in range(tok_rows // 128):
            cols[which, pl.ds(b * 128, 128), :] = jnp.transpose(ref[:, pl.ds(b * 128, 128)])

    columns(0, meta_ref)
    stages[3].wait()

    lane = lax.broadcasted_iota(jnp.int32, (1, 384), 1)
    parity = jnp.where(lane < 256, lane // 128, (lane - 256) // 64).astype(jnp.float32)
    low = lax.broadcasted_iota(jnp.int32, (1, 128), 1) < 64

    def span_of(block):
        return pl.ds(pl.multiple_of(block * height, height), height)

    def evaluate(block, ref, which, phase):
        span = span_of(block)
        tokens = ref[span, :].astype(jnp.float32)
        square = jnp.mean(tokens * tokens, axis=-1, keepdims=True)
        tokens = (tokens * lax.rsqrt(square + epsilon)).astype(jnp.bfloat16)
        ids = [cols[which, span, pl.ds(k, 1)] for k in (0, 1)]
        gate, up = [
            lax.dot_general(
                tokens, gu_all[2 * phase + kind], (((1,), (1,)), ((), ())),
                preferred_element_type=jnp.float32,
            )
            for kind in (0, 1)
        ]
        hidden = gate / (1.0 + jnp.exp(-gate)) * up
        folded = []
        for k in (0, 1):
            value = jnp.zeros((height, 384), jnp.float32)
            for pair in (0, 1):
                named = base[2 * phase + pair] + parity
                part = hidden[:, pair * 384 : (pair + 1) * 384]
                value = value + jnp.where(ids[k] == named, part, 0.0)
            folded.append(value)
        return folded

    def pick_copy(block, which, owner, kind, to):
        place = picks.at[which, owner, span_of(block), :]
        return pltpu.make_async_remote_copy(
            src_ref=place, dst_ref=place,
            send_sem=pick_send.at[which, kind, block], recv_sem=pick_recv.at[which, owner, block],
            device_id={"tp": to}, device_id_type=MESH,
        )

    def share(block, which, folded):
        span = span_of(block)
        routes = [cols[which, span, pl.ds(2 + k, 1)] for k in (0, 1)]
        folded = [folded[k] * (routes[k] / (routes[0] + routes[1])) for k in (0, 1)]
        ends = [f[:, 256:384] + pltpu.roll(f[:, 256:384], 64, 1) for f in folded]
        for k in (0, 1):
            whole = folded[k][:, :128] + folded[k][:, 128:256]
            picks[which, tp_at, span, pl.ds(k * 128, 128)] = whole.astype(jnp.bfloat16)
        picks[which, tp_at, span, pl.ds(256, 128)] = jnp.where(low, ends[0], ends[1]).astype(
            jnp.bfloat16
        )
        pick_copy(block, which, tp_at, 0, across).start()
        pick_copy(block, which, tp_at, 1, mate).start()

    def pass_on(block, which):
        pick_copy(block, which, across, 2, mate).wait_recv()
        pick_copy(block, which, across, 2, mate).start()

    def picked_up(block, which):
        pick_copy(block, which, mate, 0, mate).wait_recv()
        pick_copy(block, which, diagonal, 0, mate).wait_recv()

    def project(block, which, phase):
        span = span_of(block)
        ids = [cols[which, span, pl.ds(k, 1)] for k in (0, 1)]
        product = None
        for index in range(tp_count):
            held = picks[which, index, span, :].astype(jnp.float32)
            tail = held[:, 256:384]
            turned = pltpu.roll(tail, 64, 1)
            ends = [jnp.where(low, tail, turned), jnp.where(low, turned, tail)]
            pieces, weights = [], []
            for pair in (2 * phase, 2 * phase + 1):
                for e in (0, 1):
                    named = float(base[pair] + e)
                    pieces.append(
                        jnp.where(ids[0] == named, held[:, :128],
                                  jnp.where(ids[1] == named, held[:, 128:256], 0.0))
                    )
                    weights.append(dn_all[pair, index, e, pl.ds(0, 128), :])
                named = base[pair] + parity[:, 256:384]
                pieces.append(
                    jnp.where(ids[0] == named, ends[0], jnp.where(ids[1] == named, ends[1], 0.0))
                )
                for e in (0, 1):
                    weights.append(dn_all[pair, index, e, pl.ds(128, 64), :])
            spread = jnp.concatenate([p.astype(jnp.bfloat16) for p in pieces], axis=1)
            part = jnp.dot(
                spread, jnp.concatenate(weights, axis=0), preferred_element_type=jnp.float32
            )
            product = part if product is None else product + part
        return product

    def reply_copy(block):
        return pltpu.make_async_remote_copy(
            src_ref=reply.at[span_of(block)], dst_ref=answer.at[span_of(block)],
            send_sem=reply_send.at[block], recv_sem=reply_recv.at[block],
            device_id={"fs": E}, device_id_type=MESH,
        )

    start = 3 * parts - 2 + 2 * lag
    loop(0, start, tick)

    @pl.when(end)
    def _():
        fold[...] = jnp.zeros_like(fold)

    @pl.when(mid)
    def _():
        meta_copy.wait_recv()
        columns(1, far_meta)

    def own_first(t):
        tick(t)

        @pl.when(mid)
        def _():
            folded = evaluate(t - start, tokens_ref, 0, 0)
            span = span_of(t - start)
            for k in (0, 1):
                fold[k, span, :] = folded[k]

    loop(start, start + blocks, own_first)
    start = start + blocks

    @pl.when(mid)
    def _():
        def landed(j):
            token_copy(j, mate, 1, {"tp": mate}).wait_recv()
            token_copy(j, diagonal, 1, {"tp": mate}).wait_recv()

        loop(0, token_parts, landed)

    def far_first(t):
        tick(t)

        @pl.when(mid)
        def _():
            share(t - start, 1, evaluate(t - start, far_tokens, 1, 0))
            pl.when(t >= start + 3)(lambda: pass_on(t - start - 3, 1))

    loop(start, start + blocks, far_first)
    shared = start + 3
    start = start + blocks

    def far_passed(t):
        tick(t)
        pl.when(mid)(lambda: pass_on(t - shared, 1))

    ready = max(start + 1, 5 * parts - 2 + 2 * lag)
    loop(start, ready, far_passed)
    start = ready

    def served(part):
        span = pl.ds(pl.multiple_of(part * rows, rows), rows)
        phase = jnp.where(mid, 0, 1)
        for kind, out in ((0, serve_g), (1, serve_u)):
            out[pl.ds(0, 128), span] = gu_all[
                2 * phase + kind, pl.ds(pl.multiple_of(side * 384 + y * 128, 128), 128), span
            ]
            out[pl.ds(128, 64), span] = gu_all[
                2 * phase + kind, pl.ds(pl.multiple_of(side * 384 + 256 + y * 64, 64), 64), span
            ]

    replied = start

    def far_second(t):
        block = t - replied

        @pl.when(jnp.logical_and(mid, block < blocks))
        def _():
            pl.when(t - shared < blocks)(lambda: pass_on(t - shared, 1))
            picked_up(block, 1)
            reply[span_of(block)] = project(block, 1, 0).astype(jnp.bfloat16)
            reply_copy(block).start()

    def far_only(t):
        tick(t)
        far_second(t)

    ready = max(start, 5 * parts - 1 + 3 * lag)
    loop(start, ready, far_only)
    start = ready

    def own_second(t):
        tick(t)

        def evaluated(block):
            folded = evaluate(block, tokens_ref, 0, 1)
            span = span_of(block)
            share(block, 0, [folded[k] + fold[k, span, :] for k in (0, 1)])

        loop(2 * (t - start), 2 * (t - start) + 2, evaluated)
        far_second(t)

    loop(start, start + blocks // 2, own_second)
    start = start + blocks // 2
    ready = max(replied + blocks, units + 3 * lag)
    loop(start, ready, far_only)

    pair = jnp.where(mid, side, 2 + side)

    def serve_copy(to, owner):
        return pltpu.make_async_remote_copy(
            src_ref=dn_all.at[pair, to, y],
            dst_ref=serve_d.at[:, pl.ds(pl.multiple_of(owner * down_cols, down_cols), down_cols)],
            send_sem=serve_send.at[to], recv_sem=serve_recv.at[owner],
            device_id={"tp": to}, device_id_type=MESH,
        )

    for hop in range(1, tp_count):
        serve_copy((tp_at + hop) % tp_count, tp_at).start()
    serve_d[:, pl.ds(pl.multiple_of(tp_at * down_cols, down_cols), down_cols)] = dn_all[pair, tp_at, y]
    loop(0, n, served)

    def finish(block):
        span = span_of(block)
        picked_up(block, 0)

        @pl.when(mid)
        def _():
            total[span, :] = project(block, 0, 0)

        @pl.when(end)
        def _():
            reply_copy(block).wait_recv()
            total[span, :] = answer[span, :].astype(jnp.float32)

        mixed_ref[span, :] = (total[span, :] + project(block, 0, 1)).astype(jnp.bfloat16)

    def close(block):
        pl.when(block < blocks)(lambda: pass_on(block, 0))
        pl.when(block > 0)(lambda: finish(block - 1))


    def drained(u):
        def from_mid(u, view, wide):
            for slot in (0, 1, 3, 4):
                copy(view, u, fs_at, X, slot).wait_send()
            pl.when(u % 2 == 0)(lambda: copy(view, u, fs_at, X, 2).wait_send())
            pl.when(u % 2 == 1)(lambda: copy(view, u, fs_at, X, 5).wait_send())

            @pl.when(wide)
            def _():
                for slot in (6, 7, 8):
                    copy(view, u, fs_at, X, slot).wait_send()

        def from_end(u, view, wide):
            for slot in (0, 1, 2):
                copy(view, u, fs_at, M, slot).wait_send()

            @pl.when(wide)
            def _():
                for slot in (3, 4, 5):
                    copy(view, u, fs_at, M, slot).wait_send()

        pl.when(mid)(lambda: group(u, from_mid))
        pl.when(end)(lambda: group(u, from_end))

    loop(0, 5 * parts, drained)
    loop(0, blocks + 1, close)
    loop(5 * parts, units, drained)

    @pl.when(mid)
    def _():
        def token_drain(j):
            for kind in (1, 2, 3):
                token_copy(j, tp_at, kind, {"tp": mate}).wait_send()

        loop(0, token_parts, token_drain)

        def block_drain(b):
            reply_copy(b).wait_send()
            for kind in (0, 1, 2):
                pick_copy(b, 1, tp_at, kind, mate).wait_send()

        loop(0, blocks, block_drain)

    @pl.when(end)
    def _():
        meta_copy.wait_send()
        loop(0, token_parts, lambda j: token_copy(j, tp_at, 0, {"fs": M}).wait_send())

    def own_drain(b):
        for kind in (0, 1, 2):
            pick_copy(b, 0, tp_at, kind, mate).wait_send()

    loop(0, blocks, own_drain)
    for hop in range(1, tp_count):
        to = (tp_at + hop) % tp_count
        serve_copy(to, tp_at).wait_send()
        serve_copy(tp_at, to).wait_recv()


def laddered(tokens, norm_gain, gate_train, up_train, down_train, expert_ids, route_weights):
    experts, rows, cols = gate_train.shape
    down_rows, down_cols = down_train.shape[1:]
    n, tp_count = lax.axis_size("fs"), lax.axis_size("tp")
    tok_rows, width = tokens.shape
    blocks, parts, ahead, lag = 4, 4, 5, 1
    vmem = pl.BlockSpec(memory_space=pltpu.VMEM)
    dma = pltpu.SemaphoreType.DMA
    bf16, f32 = jnp.bfloat16, jnp.float32
    anywhere = pl.BlockSpec(memory_space=pltpu.HBM)
    units = 6 * parts
    gate_serve, up_serve, down_serve, mixed = pl.pallas_call(
        functools.partial(ladder_kernel, n, tp_count, parts, ahead, lag, blocks),
        out_shape=(
            jax.ShapeDtypeStruct((cols, width), bf16),
            jax.ShapeDtypeStruct((cols, width), bf16),
            jax.ShapeDtypeStruct((2 * down_rows, width), bf16),
            jax.ShapeDtypeStruct((tok_rows, down_cols), bf16),
        ),
        in_specs=[anywhere] * 3 + [vmem, anywhere, vmem, vmem],
        out_specs=(vmem,) * 4,
        scratch_shapes=[
            pltpu.VMEM((experts, cols, rows), f32),
            pltpu.VMEM((experts, cols, rows), f32),
            pltpu.VMEM((experts, down_rows, down_cols), f32),
            pltpu.VMEM((tok_rows, width), bf16),
            pltpu.VMEM((8, tok_rows), f32),
            dma((4,)),
            pltpu.VMEM((4, 4 * cols, width), bf16),
            pltpu.VMEM((4, tp_count, 2, 2 * down_rows, down_cols), bf16),
            pltpu.VMEM((tok_rows, width), bf16),
            pltpu.VMEM((8, tok_rows), f32),
            pltpu.VMEM((2, tok_rows, 8), f32),
            pltpu.VMEM((2, tok_rows, 384), f32),
            pltpu.VMEM((2, tp_count, tok_rows, 384), bf16),
            pltpu.VMEM((tok_rows, down_cols), f32),
            pltpu.VMEM((tok_rows, down_cols), bf16),
            pltpu.VMEM((tok_rows, down_cols), bf16),
            dma((9, units)),
            dma((n, units)),
            dma((3, 2 * parts)),
            dma((tp_count, 2 * parts)),
            dma,
            dma,
            dma((2, 3, blocks)),
            dma((2, tp_count, blocks)),
            dma((blocks,)),
            dma((blocks,)),
            dma((tp_count,)),
            dma((tp_count,)),
        ],
        compiler_params=pltpu.CompilerParams(
            collective_id=0, has_side_effects=True, vmem_limit_bytes=63 * 1024 * 1024
        ),
    )(
        gate_train.transpose(0, 2, 1), up_train.transpose(0, 2, 1), down_train,
        norm_gain[None, :], tokens, expert_ids.T, route_weights.T,
    )
    return gate_serve.T[None], up_serve.T[None], down_serve[None], mixed


def on_device(tokens, norm_gain, gate_train, up_train, down_train, expert_ids, route_weights):
    experts, rows, cols = gate_train.shape
    n, tp_count = lax.axis_size("fs"), lax.axis_size("tp")
    fits = experts == n and n == 2 * tp_count and cols == 192 and expert_ids.shape[1] == 2
    held = 3 * experts * n * rows * cols * 2
    run = laddered if fits and held < 24 * 1024 * 1024 else gathered
    return run(
        tokens, norm_gain, gate_train, up_train, down_train, expert_ids, route_weights
    )


def solution(mesh):
    return jax.shard_map(
        on_device,
        mesh=mesh,
        in_specs=(
            P("fs", None),
            P("fs"),
            P(None, "fs", "tp"),
            P(None, "fs", "tp"),
            P(None, "fs", "tp"),
            P("fs", None),
            P("fs", None),
        ),
        out_specs=(P("fs", None, "tp"), P("fs", None, "tp"), P("fs", "tp", None), P("fs", "tp")),
        check_vma=False,
    )
```

```python
import functools

import jax
import jax.numpy as jnp
from jax import lax
from jax.experimental import pallas as pl
from jax.experimental.pallas import tpu as pltpu
from jax.sharding import PartitionSpec as P

epsilon = 1e-06


def gathered(tokens, norm_gain, gate_train, up_train, down_train, expert_ids, route_weights):
    experts, rows, cols = gate_train.shape
    fs_at = lax.axis_index("fs")
    tok_rows, picks = expert_ids.shape
    down_rows, down_cols = down_train.shape[1:]
    fs_count = lax.axis_size("fs")

    gate_up = jnp.concatenate(
        [norm_gain[None, :, None] * gate_train, norm_gain[None, :, None] * up_train], axis=2
    ).astype(jnp.bfloat16)
    gate_up = gate_up.transpose(1, 0, 2).reshape(rows, experts * 2 * cols)
    gate_up_all = lax.all_gather(gate_up, "fs", axis=0, tiled=True)
    down_all = lax.all_gather(
        down_train.astype(jnp.bfloat16).reshape(experts * down_rows, down_cols),
        "fs", axis=0, tiled=True,
    )

    tok_float = tokens.astype(jnp.float32)
    normed = (
        tok_float * lax.rsqrt(jnp.mean(tok_float * tok_float, axis=-1, keepdims=True) + epsilon)
    ).astype(jnp.bfloat16)
    shares = route_weights / jnp.sum(route_weights, axis=-1, keepdims=True)

    group = 2 * lax.axis_size("tp")
    picked = [jnp.zeros((tok_rows, cols), jnp.float32) for _ in range(picks)]
    for first in range(0, experts, group):
        part = gate_up_all[:, first * 2 * cols : (first + group) * 2 * cols]
        if first:
            part, picked = lax.optimization_barrier((part, picked))
        acts = jnp.dot(normed, part, preferred_element_type=jnp.float32)
        for at in range(group):
            g = acts[:, at * 2 * cols : at * 2 * cols + cols]
            u = acts[:, at * 2 * cols + cols : (at + 1) * 2 * cols]
            h = jax.nn.silu(g) * u
            for k in range(picks):
                picked[k] = picked[k] + jnp.where(
                    expert_ids[:, k : k + 1] == first + at, h, 0.0
                )
    hidden = jnp.stack([picked[k] * shares[:, k : k + 1] for k in range(picks)], 0)
    hidden_all = lax.all_gather(hidden.astype(jnp.bfloat16), "tp", axis=2, tiled=True)
    hidden_all = hidden_all.reshape(picks, tok_rows, fs_count, 1, down_rows)
    ids = jnp.arange(experts, dtype=jnp.int32)[None, None, :, None]
    mixed = jnp.zeros((tok_rows, down_cols), jnp.float32)
    for first in range(0, fs_count, group):
        blocks = hidden_all[:, :, first : first + group]
        if first:
            blocks, mixed = lax.optimization_barrier((blocks, mixed))
        spread = jnp.zeros((tok_rows, group, experts, down_rows), jnp.bfloat16)
        for k in range(picks):
            spread = jnp.where(expert_ids[:, k][:, None, None, None] == ids, blocks[k], spread)
        depth = experts * down_rows
        mixed = mixed + jnp.dot(
            spread.reshape(tok_rows, group * depth),
            down_all[first * depth : (first + group) * depth],
            preferred_element_type=jnp.float32,
        )
    mixed = mixed.astype(jnp.bfloat16)

    own = lax.dynamic_slice_in_dim(gate_up_all, fs_at * 2 * cols, 2 * cols, 1)
    down_own = lax.dynamic_slice_in_dim(
        down_all.reshape(fs_count, experts, down_rows, down_cols), fs_at, 1, 1
    ).reshape(1, fs_count * down_rows, down_cols)
    down_serve = lax.all_to_all(down_own, "tp", split_axis=1, concat_axis=2, tiled=True)
    return own[None, :, :cols], own[None, :, cols:], down_serve, mixed


def ladder_kernel(
    n, tp_count, parts, ahead, lag, blocks, gate_in, up_in, down_in, gain_ref, tokens_in, ids_ref,
    routes_ref, serve_g, serve_u, serve_d, mixed_ref,
    gate_stage, up_stage, down_stage, tokens_ref, meta_ref, stage_sem, gu_all, dn_all, far_tokens, far_meta, cols, fold, picks, total, reply, answer,
    send_sem, recv_sem, tok_send, tok_recv, meta_send, meta_recv,
    pick_send, pick_recv, reply_send, reply_recv, serve_send, serve_recv,
):
    fs_at, tp_at = lax.axis_index("fs"), lax.axis_index("tp")
    rows = gate_in.shape[2]
    down_rows, down_cols = down_in.shape[1:]
    tok_rows = tokens_in.shape[0]
    height = tok_rows // blocks
    quarter = n // 4
    base = (quarter, 2 * quarter, 0, 3 * quarter)
    gates = 4 * parts
    units = 6 * parts
    chunk = gu_all.shape[1] // parts
    flight = send_sem.shape[1]

    z, y = fs_at // 2, fs_at % 2
    side = z // 2
    mid = jnp.logical_or(z == 1, z == 2)
    end = jnp.logical_not(mid)
    near_mid, far_mid = 1 + side, 2 - side
    near_end, far_end = 3 * side, 3 - 3 * side

    def at(zz, yy):
        return zz * 2 + yy

    E, Eo = at(near_end, y), at(near_end, 1 - y)
    M, R = at(near_mid, y), at(near_mid, 1 - y)
    X, Xo = at(far_mid, y), at(far_mid, 1 - y)
    F, Fo = at(far_end, y), at(far_end, 1 - y)
    across = tp_at + 2 - 4 * (tp_at // 2)
    mate = tp_at + 1 - 2 * (tp_at % 2)
    diagonal = across + 1 - 2 * (tp_at % 2)

    stages = [
        pltpu.make_async_copy(src, dst, stage_sem.at[k])
        for k, (src, dst) in enumerate(
            [(gate_in, gate_stage), (up_in, up_stage), (down_in, down_stage), (tokens_in, tokens_ref)]
        )
    ]
    for stage in stages:
        stage.start()

    MESH = pl.DeviceIdType.MESH
    barrier = pltpu.get_barrier_semaphore()

    def greet(to):
        pl.semaphore_signal(barrier, inc=1, device_id=to, device_id_type=MESH)

    for hop in range(1, tp_count):
        greet({"tp": (tp_at + hop) % tp_count})

    @pl.when(mid)
    def _():
        greet({"fs": E})
        greet({"fs": R})
        greet({"fs": X})

    @pl.when(end)
    def _():
        greet({"fs": M})
        greet({"fs": Eo})

    own_cols = pl.ds(pl.multiple_of(fs_at * rows, rows), rows)
    own_rows = pl.ds(pl.multiple_of((fs_at % 2) * down_rows, down_rows), down_rows)
    for kind, stage in ((0, gate_stage), (1, up_stage)):
        stages[kind].wait()
        for p in range(4):
            for i in (0, 1):
                value = (stage[base[p] + i] * gain_ref[...]).astype(jnp.bfloat16)
                top = (p % 2) * 384 + i * 128
                low_at = (p % 2) * 384 + 256 + i * 64
                gu_all[2 * (p // 2) + kind, pl.ds(top, 128), own_cols] = value[:128]
                gu_all[2 * (p // 2) + kind, pl.ds(low_at, 64), own_cols] = value[128:]
    stages[2].wait()
    for p in range(4):
        for i in (0, 1):
            dn_all[p, fs_at // 2, i, own_rows, :] = down_stage[base[p] + i].astype(jnp.bfloat16)
    meta_ref[pl.ds(0, 2), :] = ids_ref[...].astype(jnp.float32)
    meta_ref[pl.ds(2, 2), :] = routes_ref[...]
    meta_ref[pl.ds(4, 4), :] = jnp.zeros((4, tok_rows), jnp.float32)
    pl.semaphore_wait(barrier, jnp.where(mid, tp_count + 2, tp_count + 1))

    def is_down(u):
        turn = jnp.logical_and(u >= 3 * parts, u % 2 == 0)
        return jnp.logical_or(turn, u >= 5 * parts)

    def is_wide(u):
        return jnp.logical_or(jnp.logical_and(u >= parts, u % 2 == 1), u >= 5 * parts)

    def gate_at(u):
        turn = parts * (1 + u % 2) + (u - parts) // 2
        return jnp.where(u < parts, u, jnp.where(u < 3 * parts, turn, (u + 3 * parts) // 2))

    def down_at(u):
        return jnp.where(u < 5 * parts, (u - 3 * parts) // 2, u - 4 * parts)

    def wide_at(w):
        return jnp.where(w < 2 * parts, parts + 1 + 2 * w, 3 * parts + w)

    def gu_view(u, s):
        g = gate_at(u)
        return gu_all.at[
            g // parts,
            pl.ds(pl.multiple_of((g % parts) * chunk, chunk), chunk),
            pl.ds(pl.multiple_of(s * rows, rows), rows),
        ]

    def dn_view(u, s):
        v = down_at(u)
        span = pl.ds(pl.multiple_of((s % 2) * down_rows, down_rows), down_rows)
        if parts == 4:
            return dn_all.at[v // 2, s // 2, v % 2, span, :]
        return dn_all.at[v, s // 2, :, span, :]

    def copy(view, u, s, to, slot):
        place = view(u, s)
        return pltpu.make_async_remote_copy(
            src_ref=place, dst_ref=place,
            send_sem=send_sem.at[slot, u % flight], recv_sem=recv_sem.at[s, u],
            device_id={"fs": to}, device_id_type=MESH,
        )

    def launch(view, u, s, to, slot, wide_only=False):
        due = u >= flight
        if wide_only:
            due = jnp.logical_and(due, is_wide(u - flight))
        transfer = copy(view, u, s, to, slot)
        pl.when(due)(transfer.wait_send)
        transfer.start()

    def group(u, body):
        inside = jnp.logical_and(u >= 0, u < units)

        @pl.when(jnp.logical_and(inside, jnp.logical_not(is_down(u))))
        def _():
            body(u, gu_view, is_wide(u))

        @pl.when(jnp.logical_and(inside, is_down(u)))
        def _():
            body(u, dn_view, is_wide(u))

    def to_far(u, view, wide):
        launch(view, u, fs_at, R, 0)
        launch(view, u, fs_at, X, 3)

    def to_end(u, view, wide):
        launch(view, u, fs_at, E, 6, True)

    def to_mid(u, view, wide):
        launch(view, u, fs_at, M, 0)

    def to_other(u, view, wide):
        launch(view, u, fs_at, Eo, 2)

    def sends(t):
        @pl.when(mid)
        def _():
            group(t + ahead, to_far)
            pl.when(t < units // 2)(lambda: group(wide_at(t), to_end))

        @pl.when(end)
        def _():
            group(t + 2, to_mid)
            group(2 * t + 2, to_other)
            group(2 * t + 3, to_other)

    def got(view, u, s):
        copy(view, u, s, s, 0).wait_recv()

    def up_from_other(u, view, wide):
        got(view, u, Eo)
        launch(view, u, Eo, M, 1)

    def opening(u):
        pl.when(mid)(lambda: group(u, to_far))

        @pl.when(jnp.logical_and(end, u < 2))
        def _():
            group(u, to_mid)
            group(u, to_other)

    token_parts = 2 * parts
    token_rows = tok_rows // tp_count // token_parts
    token_from = 3

    def token_copy(j, owner, kind, to):
        span = pl.ds(pl.multiple_of((owner * token_parts + j) * token_rows, token_rows), token_rows)
        return pltpu.make_async_remote_copy(
            src_ref=tokens_ref.at[span] if kind == 0 else far_tokens.at[span],
            dst_ref=far_tokens.at[span],
            send_sem=tok_send.at[max(kind - 1, 0), j], recv_sem=tok_recv.at[owner, j],
            device_id=to, device_id_type=MESH,
        )

    def tick(t):
        sends(t)

        @pl.when(mid)
        def _():
            def first(u, view, wide):
                got(view, u, E)
                launch(view, u, E, X, 4)
                got(view, u, X)
                launch(view, u, X, R, 1)
                pl.when(wide)(lambda: launch(view, u, X, E, 7, True))
                got(view, u, R)

            def second(u, view, wide):
                got(view, u, Eo)
                pl.when(u % 2 == 1)(lambda: launch(view, u, Eo, X, 5))
                got(view, u, F)
                pl.when(u % 2 == 0)(lambda: launch(view, u, F, R, 2))
                pl.when(wide)(lambda: launch(view, u, F, E, 8, True))
                got(view, u, Xo)

            group(t, first)
            group(t - lag, second)
            group(t - 2 * lag, lambda u, view, wide: got(view, u, Fo))
            j = t - token_from - 2

            @pl.when(jnp.logical_and(j >= 0, j < token_parts))
            def _():
                token_copy(j, tp_at, 1, {"tp": across}).wait_recv()
                token_copy(j, tp_at, 1, {"tp": across}).start()
                token_copy(j, tp_at, 2, {"tp": mate}).start()

            i = j - 1

            @pl.when(jnp.logical_and(i >= 0, i < token_parts))
            def _():
                token_copy(i, across, 3, {"tp": mate}).wait_recv()
                token_copy(i, across, 3, {"tp": mate}).start()

        @pl.when(end)
        def _():
            def early(u, view, wide):
                got(view, u, M)
                launch(view, u, M, Eo, 3, True)

            def second(u, view, wide):
                @pl.when(wide)
                def _():
                    got(view, u, X)
                    launch(view, u, X, Eo, 4, True)

            def third(u, view, wide):
                @pl.when(wide)
                def _():
                    got(view, u, F)
                    launch(view, u, F, Eo, 5, True)
                    got(view, u, Xo)

            def fourth(u, view, wide):
                pl.when(jnp.logical_and(wide, u != 5 * parts - 1))(lambda: got(view, u, Fo))

            group(t + 2, up_from_other)
            early_at = t - 2 * parts
            pl.when(jnp.logical_and(early_at >= 0, early_at < units // 2))(
                lambda: group(wide_at(early_at), early)
            )
            late_at = early_at - 2
            pl.when(jnp.logical_and(late_at >= 0, late_at < units // 2))(
                lambda: group(wide_at(late_at), lambda u, view, wide: got(view, u, R))
            )
            group(t - lag, second)
            group(t - 2 * lag, third)
            group(t - 3 * lag, fourth)
            j = t - token_from

            @pl.when(jnp.logical_and(j >= 0, j < token_parts))
            def _():
                token_copy(j, tp_at, 0, {"fs": M}).start()

    meta_copy = pltpu.make_async_remote_copy(
        src_ref=meta_ref, dst_ref=far_meta, send_sem=meta_send, recv_sem=meta_recv,
        device_id={"fs": M}, device_id_type=MESH,
    )

    def loop(first, last, body):
        def step(t, carry):
            body(t)
            return carry

        lax.fori_loop(first, last, step, 0)

    loop(0, ahead, opening)
    pl.when(end)(meta_copy.start)

    def columns(which, ref):
        for b in range(tok_rows // 128):
            cols[which, pl.ds(b * 128, 128), :] = jnp.transpose(ref[:, pl.ds(b * 128, 128)])

    columns(0, meta_ref)
    stages[3].wait()

    lane = lax.broadcasted_iota(jnp.int32, (1, 384), 1)
    parity = jnp.where(lane < 256, lane // 128, (lane - 256) // 64).astype(jnp.float32)
    low = lax.broadcasted_iota(jnp.int32, (1, 128), 1) < 64

    def span_of(block):
        return pl.ds(pl.multiple_of(block * height, height), height)

    def evaluate(block, ref, which, phase):
        span = span_of(block)
        tokens = ref[span, :].astype(jnp.float32)
        square = jnp.mean(tokens * tokens, axis=-1, keepdims=True)
        tokens = (tokens * lax.rsqrt(square + epsilon)).astype(jnp.bfloat16)
        ids = [cols[which, span, pl.ds(k, 1)] for k in (0, 1)]
        gate, up = [
            lax.dot_general(
                tokens, gu_all[2 * phase + kind], (((1,), (1,)), ((), ())),
                preferred_element_type=jnp.float32,
            )
            for kind in (0, 1)
        ]
        hidden = gate / (1.0 + jnp.exp(-gate)) * up
        folded = []
        for k in (0, 1):
            value = jnp.zeros((height, 384), jnp.float32)
            for pair in (0, 1):
                named = base[2 * phase + pair] + parity
                part = hidden[:, pair * 384 : (pair + 1) * 384]
                value = value + jnp.where(ids[k] == named, part, 0.0)
            folded.append(value)
        return folded

    def pick_copy(block, which, owner, kind, to):
        place = picks.at[which, owner, span_of(block), :]
        return pltpu.make_async_remote_copy(
            src_ref=place, dst_ref=place,
            send_sem=pick_send.at[which, kind, block], recv_sem=pick_recv.at[which, owner, block],
            device_id={"tp": to}, device_id_type=MESH,
        )

    def share(block, which, folded):
        span = span_of(block)
        routes = [cols[which, span, pl.ds(2 + k, 1)] for k in (0, 1)]
        folded = [folded[k] * (routes[k] / (routes[0] + routes[1])) for k in (0, 1)]
        ends = [f[:, 256:384] + pltpu.roll(f[:, 256:384], 64, 1) for f in folded]
        for k in (0, 1):
            whole = folded[k][:, :128] + folded[k][:, 128:256]
            picks[which, tp_at, span, pl.ds(k * 128, 128)] = whole.astype(jnp.bfloat16)
        picks[which, tp_at, span, pl.ds(256, 128)] = jnp.where(low, ends[0], ends[1]).astype(
            jnp.bfloat16
        )
        pick_copy(block, which, tp_at, 0, across).start()
        pick_copy(block, which, tp_at, 1, mate).start()

    def pass_on(block, which):
        pick_copy(block, which, across, 2, mate).wait_recv()
        pick_copy(block, which, across, 2, mate).start()

    def picked_up(block, which):
        pick_copy(block, which, mate, 0, mate).wait_recv()
        pick_copy(block, which, diagonal, 0, mate).wait_recv()

    def project(block, which, phase):
        span = span_of(block)
        ids = [cols[which, span, pl.ds(k, 1)] for k in (0, 1)]
        product = None
        for index in range(tp_count):
            held = picks[which, index, span, :].astype(jnp.float32)
            tail = held[:, 256:384]
            turned = pltpu.roll(tail, 64, 1)
            ends = [jnp.where(low, tail, turned), jnp.where(low, turned, tail)]
            pieces, weights = [], []
            for pair in (2 * phase, 2 * phase + 1):
                for e in (0, 1):
                    named = float(base[pair] + e)
                    pieces.append(
                        jnp.where(ids[0] == named, held[:, :128],
                                  jnp.where(ids[1] == named, held[:, 128:256], 0.0))
                    )
                    weights.append(dn_all[pair, index, e, pl.ds(0, 128), :])
                named = base[pair] + parity[:, 256:384]
                pieces.append(
                    jnp.where(ids[0] == named, ends[0], jnp.where(ids[1] == named, ends[1], 0.0))
                )
                for e in (0, 1):
                    weights.append(dn_all[pair, index, e, pl.ds(128, 64), :])
            spread = jnp.concatenate([p.astype(jnp.bfloat16) for p in pieces], axis=1)
            part = jnp.dot(
                spread, jnp.concatenate(weights, axis=0), preferred_element_type=jnp.float32
            )
            product = part if product is None else product + part
        return product

    def reply_copy(block):
        return pltpu.make_async_remote_copy(
            src_ref=reply.at[span_of(block)], dst_ref=answer.at[span_of(block)],
            send_sem=reply_send.at[block], recv_sem=reply_recv.at[block],
            device_id={"fs": E}, device_id_type=MESH,
        )

    pl.when(end)(lambda: loop(0, 2, lambda u: group(u, up_from_other)))

    start = 3 * parts - 2 + 2 * lag
    loop(0, start, tick)

    @pl.when(end)
    def _():
        fold[...] = jnp.zeros_like(fold)

    @pl.when(mid)
    def _():
        meta_copy.wait_recv()
        columns(1, far_meta)

    def own_first(t):
        tick(t)

        @pl.when(mid)
        def _():
            folded = evaluate(t - start, tokens_ref, 0, 0)
            span = span_of(t - start)
            for k in (0, 1):
                fold[k, span, :] = folded[k]

    loop(start, start + blocks, own_first)
    start = start + blocks

    @pl.when(mid)
    def _():
        def landed(j):
            token_copy(j, mate, 1, {"tp": mate}).wait_recv()
            token_copy(j, diagonal, 1, {"tp": mate}).wait_recv()

        loop(0, token_parts, landed)

    def far_first(t):
        tick(t)

        @pl.when(mid)
        def _():
            share(t - start, 1, evaluate(t - start, far_tokens, 1, 0))
            pl.when(t >= start + 3)(lambda: pass_on(t - start - 3, 1))

    loop(start, start + blocks, far_first)
    shared = start + 3
    start = start + blocks

    def far_passed(t):
        tick(t)
        pl.when(mid)(lambda: pass_on(t - shared, 1))

    ready = max(start, 5 * parts - 2 + 2 * lag)
    loop(start, ready, far_passed)
    start = ready

    def served(part):
        span = pl.ds(pl.multiple_of(part * rows, rows), rows)
        phase = jnp.where(mid, 0, 1)
        for kind, out in ((0, serve_g), (1, serve_u)):
            out[pl.ds(0, 128), span] = gu_all[
                2 * phase + kind, pl.ds(pl.multiple_of(side * 384 + y * 128, 128), 128), span
            ]
            out[pl.ds(128, 64), span] = gu_all[
                2 * phase + kind, pl.ds(pl.multiple_of(side * 384 + 256 + y * 64, 64), 64), span
            ]

    replied = start

    def far_second(t):
        pl.when(jnp.logical_and(mid, t - shared < blocks))(lambda: pass_on(t - shared, 1))
        early = t - replied
        late = t - units

        def replying(block):
            picked_up(block, 1)
            reply[span_of(block)] = project(block, 1, 0).astype(jnp.bfloat16)
            reply_copy(block).start()

        first = jnp.where(early == 0, 0, 1)
        count = jnp.where(early == 0, 1, jnp.where(late == 0, blocks - 1, 0))
        pl.when(mid)(lambda: loop(first, first + count, replying))

    def far_only(t):
        tick(t)
        far_second(t)

    ready = max(start, 5 * parts - 1 + 3 * lag)
    loop(start, ready, far_only)
    start = ready

    pl.when(end)(
        lambda: group(jnp.int32(5 * parts - 1), lambda u, view, wide: got(view, u, Fo))
    )

    def own_second(t):
        def evaluated(block):
            folded = evaluate(block, tokens_ref, 0, 1)
            span = span_of(block)
            share(block, 0, [folded[k] + fold[k, span, :] for k in (0, 1)])

        loop(2 * (t - start), 2 * (t - start) + 2, evaluated)
        tick(t)
        far_second(t)

    loop(start, start + blocks // 2, own_second)
    start = start + blocks // 2
    ready = units + 3 * lag
    loop(start, ready, far_only)

    pair = jnp.where(mid, side, 2 + side)

    def serve_copy(to, owner):
        return pltpu.make_async_remote_copy(
            src_ref=dn_all.at[pair, to, y],
            dst_ref=serve_d.at[:, pl.ds(pl.multiple_of(owner * down_cols, down_cols), down_cols)],
            send_sem=serve_send.at[to], recv_sem=serve_recv.at[owner],
            device_id={"tp": to}, device_id_type=MESH,
        )

    for hop in range(1, tp_count):
        serve_copy((tp_at + hop) % tp_count, tp_at).start()
    serve_d[:, pl.ds(pl.multiple_of(tp_at * down_cols, down_cols), down_cols)] = dn_all[pair, tp_at, y]
    loop(0, n, served)

    def finish(block):
        span = span_of(block)
        picked_up(block, 0)

        total[span, :] = project(block, 0, 1)

        @pl.when(mid)
        def _():
            mixed_ref[span, :] = (total[span, :] + project(block, 0, 0)).astype(jnp.bfloat16)

        @pl.when(end)
        def _():
            reply_copy(block).wait_recv()
            mixed_ref[span, :] = (total[span, :] + answer[span, :].astype(jnp.float32)).astype(
                jnp.bfloat16
            )

    def close(block):
        pl.when(block < blocks)(lambda: pass_on(block, 0))
        pl.when(block > 0)(lambda: finish(block - 1))


    def drained(u):
        def from_mid(u, view, wide):
            for slot in (0, 1, 3, 4):
                copy(view, u, fs_at, X, slot).wait_send()
            pl.when(u % 2 == 0)(lambda: copy(view, u, fs_at, X, 2).wait_send())
            pl.when(u % 2 == 1)(lambda: copy(view, u, fs_at, X, 5).wait_send())

            @pl.when(wide)
            def _():
                for slot in (6, 7, 8):
                    copy(view, u, fs_at, X, slot).wait_send()

        def from_end(u, view, wide):
            for slot in (0, 1, 2):
                copy(view, u, fs_at, M, slot).wait_send()

            @pl.when(wide)
            def _():
                for slot in (3, 4, 5):
                    copy(view, u, fs_at, M, slot).wait_send()

        pl.when(mid)(lambda: group(u, from_mid))
        pl.when(end)(lambda: group(u, from_end))

    loop(0, blocks + 1, close)
    loop(units - flight, units, drained)

    @pl.when(mid)
    def _():
        def token_drain(j):
            for kind in (1, 2, 3):
                token_copy(j, tp_at, kind, {"tp": mate}).wait_send()

        loop(0, token_parts, token_drain)

        def block_drain(b):
            reply_copy(b).wait_send()
            for kind in (0, 1, 2):
                pick_copy(b, 1, tp_at, kind, mate).wait_send()

        loop(0, blocks, block_drain)

    @pl.when(end)
    def _():
        meta_copy.wait_send()
        loop(0, token_parts, lambda j: token_copy(j, tp_at, 0, {"fs": M}).wait_send())

    def own_drain(b):
        for kind in (0, 1, 2):
            pick_copy(b, 0, tp_at, kind, mate).wait_send()

    loop(0, blocks, own_drain)
    for hop in range(1, tp_count):
        to = (tp_at + hop) % tp_count
        serve_copy(to, tp_at).wait_send()
        serve_copy(tp_at, to).wait_recv()


def laddered(tokens, norm_gain, gate_train, up_train, down_train, expert_ids, route_weights):
    experts, rows, cols = gate_train.shape
    down_rows, down_cols = down_train.shape[1:]
    n, tp_count = lax.axis_size("fs"), lax.axis_size("tp")
    tok_rows, width = tokens.shape
    blocks, parts, ahead, lag = 4, 4, 5, 1
    vmem = pl.BlockSpec(memory_space=pltpu.VMEM)
    dma = pltpu.SemaphoreType.DMA
    bf16, f32 = jnp.bfloat16, jnp.float32
    anywhere = pl.BlockSpec(memory_space=pltpu.HBM)
    units = 6 * parts
    gate_serve, up_serve, down_serve, mixed = pl.pallas_call(
        functools.partial(ladder_kernel, n, tp_count, parts, ahead, lag, blocks),
        out_shape=(
            jax.ShapeDtypeStruct((cols, width), bf16),
            jax.ShapeDtypeStruct((cols, width), bf16),
            jax.ShapeDtypeStruct((2 * down_rows, width), bf16),
            jax.ShapeDtypeStruct((tok_rows, down_cols), bf16),
        ),
        in_specs=[anywhere] * 3 + [vmem, anywhere, vmem, vmem],
        out_specs=(vmem,) * 4,
        scratch_shapes=[
            pltpu.VMEM((experts, cols, rows), f32),
            pltpu.VMEM((experts, cols, rows), f32),
            pltpu.VMEM((experts, down_rows, down_cols), f32),
            pltpu.VMEM((tok_rows, width), bf16),
            pltpu.VMEM((8, tok_rows), f32),
            dma((4,)),
            pltpu.VMEM((4, 4 * cols, width), bf16),
            pltpu.VMEM((4, tp_count, 2, 2 * down_rows, down_cols), bf16),
            pltpu.VMEM((tok_rows, width), bf16),
            pltpu.VMEM((8, tok_rows), f32),
            pltpu.VMEM((2, tok_rows, 8), f32),
            pltpu.VMEM((2, tok_rows, 384), f32),
            pltpu.VMEM((2, tp_count, tok_rows, 384), bf16),
            pltpu.VMEM((tok_rows, down_cols), f32),
            pltpu.VMEM((tok_rows, down_cols), bf16),
            pltpu.VMEM((tok_rows, down_cols), bf16),
            dma((9, 2 * parts)),
            dma((n, units)),
            dma((3, 2 * parts)),
            dma((tp_count, 2 * parts)),
            dma,
            dma,
            dma((2, 3, blocks)),
            dma((2, tp_count, blocks)),
            dma((blocks,)),
            dma((blocks,)),
            dma((tp_count,)),
            dma((tp_count,)),
        ],
        compiler_params=pltpu.CompilerParams(
            collective_id=0, has_side_effects=True, vmem_limit_bytes=50 * 1024 * 1024
        ),
    )(
        gate_train.transpose(0, 2, 1), up_train.transpose(0, 2, 1), down_train,
        norm_gain[None, :], tokens, expert_ids.T, route_weights.T,
    )
    return gate_serve.T[None], up_serve.T[None], down_serve[None], mixed


def on_device(tokens, norm_gain, gate_train, up_train, down_train, expert_ids, route_weights):
    experts, rows, cols = gate_train.shape
    n, tp_count = lax.axis_size("fs"), lax.axis_size("tp")
    fits = experts == n and n == 2 * tp_count and cols == 192 and expert_ids.shape[1] == 2
    held = 3 * experts * n * rows * cols * 2
    run = laddered if fits and held < 24 * 1024 * 1024 else gathered
    return run(
        tokens, norm_gain, gate_train, up_train, down_train, expert_ids, route_weights
    )


def solution(mesh):
    return jax.shard_map(
        on_device,
        mesh=mesh,
        in_specs=(
            P("fs", None),
            P("fs"),
            P(None, "fs", "tp"),
            P(None, "fs", "tp"),
            P(None, "fs", "tp"),
            P("fs", None),
            P("fs", None),
        ),
        out_specs=(P("fs", None, "tp"), P("fs", None, "tp"), P("fs", "tp", None), P("fs", "tp")),
        check_vma=False,
    )
```

```python
import functools

import jax
import jax.numpy as jnp
from jax import lax
from jax.experimental import pallas as pl
from jax.experimental.pallas import tpu as pltpu
from jax.sharding import PartitionSpec as P

epsilon = 1e-06


def gathered(tokens, norm_gain, gate_train, up_train, down_train, expert_ids, route_weights):
    experts, rows, cols = gate_train.shape
    fs_at = lax.axis_index("fs")
    tok_rows, picks = expert_ids.shape
    down_rows, down_cols = down_train.shape[1:]
    fs_count = lax.axis_size("fs")

    gate_up = jnp.concatenate(
        [norm_gain[None, :, None] * gate_train, norm_gain[None, :, None] * up_train], axis=2
    ).astype(jnp.bfloat16)
    gate_up = gate_up.transpose(1, 0, 2).reshape(rows, experts * 2 * cols)
    gate_up_all = lax.all_gather(gate_up, "fs", axis=0, tiled=True)
    down_all = lax.all_gather(
        down_train.astype(jnp.bfloat16).reshape(experts * down_rows, down_cols),
        "fs", axis=0, tiled=True,
    )

    tok_float = tokens.astype(jnp.float32)
    normed = (
        tok_float * lax.rsqrt(jnp.mean(tok_float * tok_float, axis=-1, keepdims=True) + epsilon)
    ).astype(jnp.bfloat16)
    shares = route_weights / jnp.sum(route_weights, axis=-1, keepdims=True)

    group = 2 * lax.axis_size("tp")
    picked = [jnp.zeros((tok_rows, cols), jnp.float32) for _ in range(picks)]
    for first in range(0, experts, group):
        part = gate_up_all[:, first * 2 * cols : (first + group) * 2 * cols]
        if first:
            part, picked = lax.optimization_barrier((part, picked))
        acts = jnp.dot(normed, part, preferred_element_type=jnp.float32)
        for at in range(group):
            g = acts[:, at * 2 * cols : at * 2 * cols + cols]
            u = acts[:, at * 2 * cols + cols : (at + 1) * 2 * cols]
            h = jax.nn.silu(g) * u
            for k in range(picks):
                picked[k] = picked[k] + jnp.where(
                    expert_ids[:, k : k + 1] == first + at, h, 0.0
                )
    hidden = jnp.stack([picked[k] * shares[:, k : k + 1] for k in range(picks)], 0)
    hidden_all = lax.all_gather(hidden.astype(jnp.bfloat16), "tp", axis=2, tiled=True)
    hidden_all = hidden_all.reshape(picks, tok_rows, fs_count, 1, down_rows)
    ids = jnp.arange(experts, dtype=jnp.int32)[None, None, :, None]
    mixed = jnp.zeros((tok_rows, down_cols), jnp.float32)
    for first in range(0, fs_count, group):
        blocks = hidden_all[:, :, first : first + group]
        if first:
            blocks, mixed = lax.optimization_barrier((blocks, mixed))
        spread = jnp.zeros((tok_rows, group, experts, down_rows), jnp.bfloat16)
        for k in range(picks):
            spread = jnp.where(expert_ids[:, k][:, None, None, None] == ids, blocks[k], spread)
        depth = experts * down_rows
        mixed = mixed + jnp.dot(
            spread.reshape(tok_rows, group * depth),
            down_all[first * depth : (first + group) * depth],
            preferred_element_type=jnp.float32,
        )
    mixed = mixed.astype(jnp.bfloat16)

    own = lax.dynamic_slice_in_dim(gate_up_all, fs_at * 2 * cols, 2 * cols, 1)
    down_own = lax.dynamic_slice_in_dim(
        down_all.reshape(fs_count, experts, down_rows, down_cols), fs_at, 1, 1
    ).reshape(1, fs_count * down_rows, down_cols)
    down_serve = lax.all_to_all(down_own, "tp", split_axis=1, concat_axis=2, tiled=True)
    return own[None, :, :cols], own[None, :, cols:], down_serve, mixed


def ladder_kernel(
    n, tp_count, parts, ahead, lag, blocks, gate_in, up_in, down_in, gain_ref, tokens_in, ids_ref,
    routes_ref, serve_g, serve_u, serve_d, mixed_ref,
    gate_stage, up_stage, down_stage, tokens_ref, meta_ref, stage_sem, gu_all, dn_all, far_tokens, far_meta, cols, fold, picks, total, reply, answer,
    send_sem, recv_sem, tok_send, tok_recv, meta_send, meta_recv,
    pick_send, pick_recv, reply_send, reply_recv, serve_send, serve_recv,
):
    fs_at, tp_at = lax.axis_index("fs"), lax.axis_index("tp")
    rows = gate_in.shape[2]
    down_rows, down_cols = down_in.shape[1:]
    tok_rows = tokens_in.shape[0]
    height = tok_rows // blocks
    quarter = n // 4
    base = (quarter, 2 * quarter, 0, 3 * quarter)
    gates = 4 * parts
    units = 6 * parts
    chunk = gu_all.shape[1] // parts
    flight = send_sem.shape[1]

    z, y = fs_at // 2, fs_at % 2
    side = z // 2
    mid = jnp.logical_or(z == 1, z == 2)
    end = jnp.logical_not(mid)
    near_mid, far_mid = 1 + side, 2 - side
    near_end, far_end = 3 * side, 3 - 3 * side

    def at(zz, yy):
        return zz * 2 + yy

    E, Eo = at(near_end, y), at(near_end, 1 - y)
    M, R = at(near_mid, y), at(near_mid, 1 - y)
    X, Xo = at(far_mid, y), at(far_mid, 1 - y)
    F, Fo = at(far_end, y), at(far_end, 1 - y)
    across = tp_at + 2 - 4 * (tp_at // 2)
    mate = tp_at + 1 - 2 * (tp_at % 2)
    diagonal = across + 1 - 2 * (tp_at % 2)

    stages = [
        pltpu.make_async_copy(src, dst, stage_sem.at[k])
        for k, (src, dst) in enumerate(
            [(gate_in, gate_stage), (up_in, up_stage), (down_in, down_stage), (tokens_in, tokens_ref)]
        )
    ]
    for stage in stages:
        stage.start()

    MESH = pl.DeviceIdType.MESH
    barrier = pltpu.get_barrier_semaphore()

    def greet(to):
        pl.semaphore_signal(barrier, inc=1, device_id=to, device_id_type=MESH)

    for hop in range(1, tp_count):
        greet({"tp": (tp_at + hop) % tp_count})

    @pl.when(mid)
    def _():
        greet({"fs": E})
        greet({"fs": R})
        greet({"fs": X})

    @pl.when(end)
    def _():
        greet({"fs": M})
        greet({"fs": Eo})

    own_cols = pl.ds(pl.multiple_of(fs_at * rows, rows), rows)
    own_rows = pl.ds(pl.multiple_of((fs_at % 2) * down_rows, down_rows), down_rows)
    for kind, stage in ((0, gate_stage), (1, up_stage)):
        stages[kind].wait()
        for p in range(4):
            for i in (0, 1):
                value = (stage[base[p] + i] * gain_ref[...]).astype(jnp.bfloat16)
                top = (p % 2) * 384 + i * 128
                low_at = (p % 2) * 384 + 256 + i * 64
                gu_all[2 * (p // 2) + kind, pl.ds(top, 128), own_cols] = value[:128]
                gu_all[2 * (p // 2) + kind, pl.ds(low_at, 64), own_cols] = value[128:]
    stages[2].wait()
    for p in range(4):
        for i in (0, 1):
            dn_all[p, fs_at // 2, i, own_rows, :] = down_stage[base[p] + i].astype(jnp.bfloat16)
    meta_ref[pl.ds(0, 2), :] = ids_ref[...].astype(jnp.float32)
    meta_ref[pl.ds(2, 2), :] = routes_ref[...]
    meta_ref[pl.ds(4, 4), :] = jnp.zeros((4, tok_rows), jnp.float32)
    pl.semaphore_wait(barrier, jnp.where(mid, tp_count + 2, tp_count + 1))

    def is_down(u):
        turn = jnp.logical_and(u >= 3 * parts, u % 2 == 0)
        return jnp.logical_or(turn, u >= 5 * parts)

    def is_wide(u):
        return jnp.logical_or(jnp.logical_and(u >= parts, u % 2 == 1), u >= 5 * parts)

    def gate_at(u):
        turn = parts * (1 + u % 2) + (u - parts) // 2
        return jnp.where(u < parts, u, jnp.where(u < 3 * parts, turn, (u + 3 * parts) // 2))

    def down_at(u):
        return jnp.where(u < 5 * parts, (u - 3 * parts) // 2, u - 4 * parts)

    def wide_at(w):
        return jnp.where(w < 2 * parts, parts + 1 + 2 * w, 3 * parts + w)

    def gu_view(u, s):
        g = gate_at(u)
        return gu_all.at[
            g // parts,
            pl.ds(pl.multiple_of((g % parts) * chunk, chunk), chunk),
            pl.ds(pl.multiple_of(s * rows, rows), rows),
        ]

    def dn_view(u, s):
        v = down_at(u)
        span = pl.ds(pl.multiple_of((s % 2) * down_rows, down_rows), down_rows)
        if parts == 4:
            return dn_all.at[v // 2, s // 2, v % 2, span, :]
        return dn_all.at[v, s // 2, :, span, :]

    def copy(view, u, s, to, slot):
        place = view(u, s)
        return pltpu.make_async_remote_copy(
            src_ref=place, dst_ref=place,
            send_sem=send_sem.at[slot, u % flight], recv_sem=recv_sem.at[s, u],
            device_id={"fs": to}, device_id_type=MESH,
        )

    def launch(view, u, s, to, slot, wide_only=False):
        due = u >= flight
        if wide_only:
            due = jnp.logical_and(due, is_wide(u - flight))
        transfer = copy(view, u, s, to, slot)
        pl.when(due)(transfer.wait_send)
        transfer.start()

    def group(u, body):
        inside = jnp.logical_and(u >= 0, u < units)

        @pl.when(jnp.logical_and(inside, jnp.logical_not(is_down(u))))
        def _():
            body(u, gu_view, is_wide(u))

        @pl.when(jnp.logical_and(inside, is_down(u)))
        def _():
            body(u, dn_view, is_wide(u))

    def to_far(u, view, wide):
        launch(view, u, fs_at, R, 0)
        launch(view, u, fs_at, X, 3)

    def to_end(u, view, wide):
        launch(view, u, fs_at, E, 6, True)

    def to_mid(u, view, wide):
        launch(view, u, fs_at, M, 0)

    def to_other(u, view, wide):
        launch(view, u, fs_at, Eo, 2)

    def sends(t):
        @pl.when(mid)
        def _():
            group(t + ahead, to_far)
            pl.when(t < units // 2)(lambda: group(wide_at(t), to_end))

        @pl.when(end)
        def _():
            group(t + 2, to_mid)
            group(2 * t + 2, to_other)
            group(2 * t + 3, to_other)

    def got(view, u, s):
        copy(view, u, s, s, 0).wait_recv()

    def up_from_other(u, view, wide):
        got(view, u, Eo)
        launch(view, u, Eo, M, 1)

    def opening(u):
        pl.when(mid)(lambda: group(u, to_far))

        @pl.when(jnp.logical_and(end, u < 2))
        def _():
            group(u, to_mid)
            group(u, to_other)

    token_parts = 2 * parts
    token_rows = tok_rows // tp_count // token_parts
    token_from = 3

    def token_copy(j, owner, kind, to):
        span = pl.ds(pl.multiple_of((owner * token_parts + j) * token_rows, token_rows), token_rows)
        return pltpu.make_async_remote_copy(
            src_ref=tokens_ref.at[span] if kind == 0 else far_tokens.at[span],
            dst_ref=far_tokens.at[span],
            send_sem=tok_send.at[max(kind - 1, 0), j], recv_sem=tok_recv.at[owner, j],
            device_id=to, device_id_type=MESH,
        )

    def tick(t):
        sends(t)

        @pl.when(mid)
        def _():
            def first(u, view, wide):
                got(view, u, E)
                launch(view, u, E, X, 4)
                got(view, u, X)
                launch(view, u, X, R, 1)
                pl.when(wide)(lambda: launch(view, u, X, E, 7, True))
                got(view, u, R)

            def second(u, view, wide):
                got(view, u, Eo)
                pl.when(u % 2 == 1)(lambda: launch(view, u, Eo, X, 5))
                got(view, u, F)
                pl.when(u % 2 == 0)(lambda: launch(view, u, F, R, 2))
                pl.when(wide)(lambda: launch(view, u, F, E, 8, True))
                got(view, u, Xo)

            group(t, first)
            group(t - lag, second)
            group(t - 2 * lag, lambda u, view, wide: got(view, u, Fo))
            j = t - token_from - 2

            @pl.when(jnp.logical_and(j >= 0, j < token_parts))
            def _():
                token_copy(j, tp_at, 1, {"tp": across}).wait_recv()
                token_copy(j, tp_at, 1, {"tp": across}).start()
                token_copy(j, tp_at, 2, {"tp": mate}).start()

            i = j - 1

            @pl.when(jnp.logical_and(i >= 0, i < token_parts))
            def _():
                token_copy(i, across, 3, {"tp": mate}).wait_recv()
                token_copy(i, across, 3, {"tp": mate}).start()

        @pl.when(end)
        def _():
            def early(u, view, wide):
                got(view, u, M)
                launch(view, u, M, Eo, 3, True)

            def second(u, view, wide):
                @pl.when(wide)
                def _():
                    got(view, u, X)
                    launch(view, u, X, Eo, 4, True)

            def third(u, view, wide):
                @pl.when(wide)
                def _():
                    got(view, u, F)
                    launch(view, u, F, Eo, 5, True)
                    got(view, u, Xo)

            def fourth(u, view, wide):
                pl.when(jnp.logical_and(wide, u != 5 * parts - 1))(lambda: got(view, u, Fo))

            group(t + 2, up_from_other)
            early_at = t - 2 * parts
            pl.when(jnp.logical_and(early_at >= 0, early_at < units // 2))(
                lambda: group(wide_at(early_at), early)
            )
            late_at = early_at - 2
            pl.when(jnp.logical_and(late_at >= 0, late_at < units // 2))(
                lambda: group(wide_at(late_at), lambda u, view, wide: got(view, u, R))
            )
            group(t - lag, second)
            group(t - 2 * lag, third)
            group(t - 3 * lag, fourth)
            j = t - token_from

            @pl.when(jnp.logical_and(j >= 0, j < token_parts))
            def _():
                token_copy(j, tp_at, 0, {"fs": M}).start()

    meta_copy = pltpu.make_async_remote_copy(
        src_ref=meta_ref, dst_ref=far_meta, send_sem=meta_send, recv_sem=meta_recv,
        device_id={"fs": M}, device_id_type=MESH,
    )

    def loop(first, last, body):
        def step(t, carry):
            body(t)
            return carry

        lax.fori_loop(first, last, step, 0)

    loop(0, ahead, opening)
    pl.when(end)(meta_copy.start)

    def columns(which, ref):
        for b in range(tok_rows // 128):
            cols[which, pl.ds(b * 128, 128), :] = jnp.transpose(ref[:, pl.ds(b * 128, 128)])

    columns(0, meta_ref)
    stages[3].wait()

    lane = lax.broadcasted_iota(jnp.int32, (1, 384), 1)
    parity = jnp.where(lane < 256, lane // 128, (lane - 256) // 64).astype(jnp.float32)
    low = lax.broadcasted_iota(jnp.int32, (1, 128), 1) < 64

    def span_of(block):
        return pl.ds(pl.multiple_of(block * height, height), height)

    def evaluate(block, ref, which, phase):
        span = span_of(block)
        tokens = ref[span, :].astype(jnp.float32)
        square = jnp.mean(tokens * tokens, axis=-1, keepdims=True)
        tokens = (tokens * lax.rsqrt(square + epsilon)).astype(jnp.bfloat16)
        ids = [cols[which, span, pl.ds(k, 1)] for k in (0, 1)]
        gate, up = [
            lax.dot_general(
                tokens, gu_all[2 * phase + kind], (((1,), (1,)), ((), ())),
                preferred_element_type=jnp.float32,
            )
            for kind in (0, 1)
        ]
        hidden = gate / (1.0 + jnp.exp(-gate)) * up
        folded = []
        for k in (0, 1):
            value = jnp.zeros((height, 384), jnp.float32)
            for pair in (0, 1):
                named = base[2 * phase + pair] + parity
                part = hidden[:, pair * 384 : (pair + 1) * 384]
                value = value + jnp.where(ids[k] == named, part, 0.0)
            folded.append(value)
        return folded

    def pick_copy(block, which, owner, kind, to):
        place = picks.at[which, owner, span_of(block), :]
        return pltpu.make_async_remote_copy(
            src_ref=place, dst_ref=place,
            send_sem=pick_send.at[which, kind, block], recv_sem=pick_recv.at[which, owner, block],
            device_id={"tp": to}, device_id_type=MESH,
        )

    def share(block, which, folded):
        span = span_of(block)
        routes = [cols[which, span, pl.ds(2 + k, 1)] for k in (0, 1)]
        folded = [folded[k] * (routes[k] / (routes[0] + routes[1])) for k in (0, 1)]
        ends = [f[:, 256:384] + pltpu.roll(f[:, 256:384], 64, 1) for f in folded]
        for k in (0, 1):
            whole = folded[k][:, :128] + folded[k][:, 128:256]
            picks[which, tp_at, span, pl.ds(k * 128, 128)] = whole.astype(jnp.bfloat16)
        picks[which, tp_at, span, pl.ds(256, 128)] = jnp.where(low, ends[0], ends[1]).astype(
            jnp.bfloat16
        )
        pick_copy(block, which, tp_at, 0, across).start()
        pick_copy(block, which, tp_at, 1, mate).start()

    def pass_on(block, which):
        pick_copy(block, which, across, 2, mate).wait_recv()
        pick_copy(block, which, across, 2, mate).start()

    def picked_up(block, which):
        pick_copy(block, which, mate, 0, mate).wait_recv()
        pick_copy(block, which, diagonal, 0, mate).wait_recv()

    def project(block, which, phase):
        span = span_of(block)
        ids = [cols[which, span, pl.ds(k, 1)] for k in (0, 1)]
        product = None
        for index in range(tp_count):
            held = picks[which, index, span, :].astype(jnp.float32)
            tail = held[:, 256:384]
            turned = pltpu.roll(tail, 64, 1)
            ends = [jnp.where(low, tail, turned), jnp.where(low, turned, tail)]
            pieces, weights = [], []
            for pair in (2 * phase, 2 * phase + 1):
                for e in (0, 1):
                    named = float(base[pair] + e)
                    pieces.append(
                        jnp.where(ids[0] == named, held[:, :128],
                                  jnp.where(ids[1] == named, held[:, 128:256], 0.0))
                    )
                    weights.append(dn_all[pair, index, e, pl.ds(0, 128), :])
                named = base[pair] + parity[:, 256:384]
                pieces.append(
                    jnp.where(ids[0] == named, ends[0], jnp.where(ids[1] == named, ends[1], 0.0))
                )
                for e in (0, 1):
                    weights.append(dn_all[pair, index, e, pl.ds(128, 64), :])
            spread = jnp.concatenate([p.astype(jnp.bfloat16) for p in pieces], axis=1)
            part = jnp.dot(
                spread, jnp.concatenate(weights, axis=0), preferred_element_type=jnp.float32
            )
            product = part if product is None else product + part
        return product

    def reply_copy(block):
        return pltpu.make_async_remote_copy(
            src_ref=reply.at[span_of(block)], dst_ref=answer.at[span_of(block)],
            send_sem=reply_send.at[block], recv_sem=reply_recv.at[block],
            device_id={"fs": E}, device_id_type=MESH,
        )

    pl.when(end)(lambda: loop(0, 2, lambda u: group(u, up_from_other)))

    start = 3 * parts - 2 + 2 * lag
    loop(0, start, tick)

    @pl.when(end)
    def _():
        fold[...] = jnp.zeros_like(fold)

    @pl.when(mid)
    def _():
        meta_copy.wait_recv()
        columns(1, far_meta)

    def own_first(t):
        tick(t)

        @pl.when(mid)
        def _():
            folded = evaluate(t - start, tokens_ref, 0, 0)
            span = span_of(t - start)
            for k in (0, 1):
                fold[k, span, :] = folded[k]

    loop(start, start + blocks, own_first)
    start = start + blocks

    @pl.when(mid)
    def _():
        def landed(j):
            token_copy(j, mate, 1, {"tp": mate}).wait_recv()
            token_copy(j, diagonal, 1, {"tp": mate}).wait_recv()

        loop(0, token_parts, landed)

    def far_first(t):
        tick(t)

        @pl.when(mid)
        def _():
            share(t - start, 1, evaluate(t - start, far_tokens, 1, 0))
            pl.when(t >= start + 3)(lambda: pass_on(t - start - 3, 1))

    loop(start, start + blocks, far_first)
    shared = start + 3
    start = start + blocks

    def far_passed(t):
        tick(t)
        pl.when(mid)(lambda: pass_on(t - shared, 1))

    ready = max(start, 5 * parts - 2 + 2 * lag)
    loop(start, ready, far_passed)
    start = ready

    def served(part):
        span = pl.ds(pl.multiple_of(part * rows, rows), rows)
        phase = jnp.where(mid, 0, 1)
        for kind, out in ((0, serve_g), (1, serve_u)):
            out[pl.ds(0, 128), span] = gu_all[
                2 * phase + kind, pl.ds(pl.multiple_of(side * 384 + y * 128, 128), 128), span
            ]
            out[pl.ds(128, 64), span] = gu_all[
                2 * phase + kind, pl.ds(pl.multiple_of(side * 384 + 256 + y * 64, 64), 64), span
            ]

    replied = start

    def far_second(t):
        pl.when(jnp.logical_and(mid, t - shared < blocks))(lambda: pass_on(t - shared, 1))
        early = t - replied
        late = t - units

        def replying(block):
            picked_up(block, 1)
            reply[span_of(block)] = project(block, 1, 0).astype(jnp.bfloat16)
            reply_copy(block).start()

        first = jnp.where(early == 0, 0, 1)
        count = jnp.where(early == 0, 1, jnp.where(late == 0, blocks - 1, 0))
        pl.when(mid)(lambda: loop(first, first + count, replying))

    def far_only(t):
        tick(t)
        far_second(t)

    ready = max(start, 5 * parts - 1 + 3 * lag)
    loop(start, ready, far_only)
    start = ready

    pl.when(end)(
        lambda: group(jnp.int32(5 * parts - 1), lambda u, view, wide: got(view, u, Fo))
    )

    def own_second(t):
        def evaluated(block):
            folded = evaluate(block, tokens_ref, 0, 1)
            span = span_of(block)
            share(block, 0, [folded[k] + fold[k, span, :] for k in (0, 1)])

        loop(2 * (t - start), 2 * (t - start) + 2, evaluated)
        tick(t)
        far_second(t)

    loop(start, start + blocks // 2, own_second)
    start = start + blocks // 2
    ready = units + 3 * lag
    loop(start, ready, far_only)

    pair = jnp.where(mid, side, 2 + side)

    def serve_copy(to, owner):
        return pltpu.make_async_remote_copy(
            src_ref=dn_all.at[pair, to, y],
            dst_ref=serve_d.at[:, pl.ds(pl.multiple_of(owner * down_cols, down_cols), down_cols)],
            send_sem=serve_send.at[to], recv_sem=serve_recv.at[owner],
            device_id={"tp": to}, device_id_type=MESH,
        )

    for hop in range(1, tp_count):
        serve_copy((tp_at + hop) % tp_count, tp_at).start()
    serve_d[:, pl.ds(pl.multiple_of(tp_at * down_cols, down_cols), down_cols)] = dn_all[pair, tp_at, y]
    loop(0, n, served)

    def finish(block):
        span = span_of(block)
        picked_up(block, 0)

        total[span, :] = project(block, 0, 1)

        @pl.when(mid)
        def _():
            mixed_ref[span, :] = (total[span, :] + project(block, 0, 0)).astype(jnp.bfloat16)

        @pl.when(end)
        def _():
            reply_copy(block).wait_recv()
            mixed_ref[span, :] = (total[span, :] + answer[span, :].astype(jnp.float32)).astype(
                jnp.bfloat16
            )

    def close(block):
        pl.when(block < blocks)(lambda: pass_on(block, 0))
        pl.when(block > 0)(lambda: finish(block - 1))


    def drained(u):
        def from_mid(u, view, wide):
            for slot in (0, 1, 3, 4):
                copy(view, u, fs_at, X, slot).wait_send()
            pl.when(u % 2 == 0)(lambda: copy(view, u, fs_at, X, 2).wait_send())
            pl.when(u % 2 == 1)(lambda: copy(view, u, fs_at, X, 5).wait_send())

            @pl.when(wide)
            def _():
                for slot in (6, 7, 8):
                    copy(view, u, fs_at, X, slot).wait_send()

        def from_end(u, view, wide):
            for slot in (0, 1, 2):
                copy(view, u, fs_at, M, slot).wait_send()

            @pl.when(wide)
            def _():
                for slot in (3, 4, 5):
                    copy(view, u, fs_at, M, slot).wait_send()

        pl.when(mid)(lambda: group(u, from_mid))
        pl.when(end)(lambda: group(u, from_end))

    loop(0, blocks + 1, close)
    loop(units - flight, units, drained)

    @pl.when(mid)
    def _():
        def token_drain(j):
            for kind in (1, 2, 3):
                token_copy(j, tp_at, kind, {"tp": mate}).wait_send()

        loop(0, token_parts, token_drain)

        def block_drain(b):
            reply_copy(b).wait_send()
            for kind in (0, 1, 2):
                pick_copy(b, 1, tp_at, kind, mate).wait_send()

        loop(0, blocks, block_drain)

    @pl.when(end)
    def _():
        meta_copy.wait_send()
        loop(0, token_parts, lambda j: token_copy(j, tp_at, 0, {"fs": M}).wait_send())

    def own_drain(b):
        for kind in (0, 1, 2):
            pick_copy(b, 0, tp_at, kind, mate).wait_send()

    loop(0, blocks, own_drain)
    for hop in range(1, tp_count):
        to = (tp_at + hop) % tp_count
        serve_copy(to, tp_at).wait_send()
        serve_copy(tp_at, to).wait_recv()


def store_kernel(*refs):
    copies = [
        pltpu.make_async_copy(refs[k], refs[4 + k], refs[8].at[k]) for k in range(4)
    ]
    for copy in copies:
        copy.start()
    for copy in copies:
        copy.wait()


def laddered(tokens, norm_gain, gate_train, up_train, down_train, expert_ids, route_weights):
    experts, rows, cols = gate_train.shape
    down_rows, down_cols = down_train.shape[1:]
    n, tp_count = lax.axis_size("fs"), lax.axis_size("tp")
    tok_rows, width = tokens.shape
    blocks, parts, ahead, lag = 4, 4, 5, 1
    vmem = pl.BlockSpec(memory_space=pltpu.VMEM)
    dma = pltpu.SemaphoreType.DMA
    bf16, f32 = jnp.bfloat16, jnp.float32
    anywhere = pl.BlockSpec(memory_space=pltpu.HBM)
    units = 6 * parts
    gate_serve, up_serve, down_serve, mixed = pl.pallas_call(
        functools.partial(ladder_kernel, n, tp_count, parts, ahead, lag, blocks),
        out_shape=(
            jax.ShapeDtypeStruct((cols, width), bf16),
            jax.ShapeDtypeStruct((cols, width), bf16),
            jax.ShapeDtypeStruct((2 * down_rows, width), bf16),
            jax.ShapeDtypeStruct((tok_rows, down_cols), bf16),
        ),
        in_specs=[anywhere] * 3 + [vmem, anywhere, vmem, vmem],
        out_specs=(vmem,) * 4,
        scratch_shapes=[
            pltpu.VMEM((experts, cols, rows), f32),
            pltpu.VMEM((experts, cols, rows), f32),
            pltpu.VMEM((experts, down_rows, down_cols), f32),
            pltpu.VMEM((tok_rows, width), bf16),
            pltpu.VMEM((8, tok_rows), f32),
            dma((4,)),
            pltpu.VMEM((4, 4 * cols, width), bf16),
            pltpu.VMEM((4, tp_count, 2, 2 * down_rows, down_cols), bf16),
            pltpu.VMEM((tok_rows, width), bf16),
            pltpu.VMEM((8, tok_rows), f32),
            pltpu.VMEM((2, tok_rows, 8), f32),
            pltpu.VMEM((2, tok_rows, 384), f32),
            pltpu.VMEM((2, tp_count, tok_rows, 384), bf16),
            pltpu.VMEM((tok_rows, down_cols), f32),
            pltpu.VMEM((tok_rows, down_cols), bf16),
            pltpu.VMEM((tok_rows, down_cols), bf16),
            dma((9, 2 * parts)),
            dma((n, units)),
            dma((3, 2 * parts)),
            dma((tp_count, 2 * parts)),
            dma,
            dma,
            dma((2, 3, blocks)),
            dma((2, tp_count, blocks)),
            dma((blocks,)),
            dma((blocks,)),
            dma((tp_count,)),
            dma((tp_count,)),
        ],
        compiler_params=pltpu.CompilerParams(
            collective_id=0, has_side_effects=True, vmem_limit_bytes=50 * 1024 * 1024
        ),
    )(
        gate_train.transpose(0, 2, 1), up_train.transpose(0, 2, 1), down_train,
        norm_gain[None, :], tokens, expert_ids.T, route_weights.T,
    )
    results = (gate_serve, up_serve, down_serve, mixed)
    gate_serve, up_serve, down_serve, mixed = pl.pallas_call(
        store_kernel,
        out_shape=tuple(jax.ShapeDtypeStruct(r.shape, r.dtype) for r in results),
        in_specs=[pl.BlockSpec(memory_space=pl.ANY)] * 4,
        out_specs=(anywhere,) * 4,
        scratch_shapes=[dma((4,))],
        compiler_params=pltpu.CompilerParams(vmem_limit_bytes=1024 * 1024),
    )(*results)
    return gate_serve.T[None], up_serve.T[None], down_serve[None], mixed


def on_device(tokens, norm_gain, gate_train, up_train, down_train, expert_ids, route_weights):
    experts, rows, cols = gate_train.shape
    n, tp_count = lax.axis_size("fs"), lax.axis_size("tp")
    fits = experts == n and n == 2 * tp_count and cols == 192 and expert_ids.shape[1] == 2
    held = 3 * experts * n * rows * cols * 2
    run = laddered if fits and held < 24 * 1024 * 1024 else gathered
    return run(
        tokens, norm_gain, gate_train, up_train, down_train, expert_ids, route_weights
    )


def solution(mesh):
    return jax.shard_map(
        on_device,
        mesh=mesh,
        in_specs=(
            P("fs", None),
            P("fs"),
            P(None, "fs", "tp"),
            P(None, "fs", "tp"),
            P(None, "fs", "tp"),
            P("fs", None),
            P("fs", None),
        ),
        out_specs=(P("fs", None, "tp"), P("fs", None, "tp"), P("fs", "tp", None), P("fs", "tp")),
        check_vma=False,
    )
```
